32 devices in a mesh: kv: 16 (over z, y, x), tp: 2 (over core).
Axes of the slice: x: 2, y: 2, z: 4, core: 2. Of those that a mesh axis runs over, the one named last changes fastest.
Arguments:
- tokens: bfloat16 [6144, 2048], P('kv', 'tp'), may hold values from -12 to 12
- query_weight: bfloat16 [2048, 2048], P(None, 'tp'), may hold values from -0.5 to 0.5
- key_weight: bfloat16 [2048, 1024], P(None, 'tp'), may hold values from -0.5 to 0.5
- value_weight: bfloat16 [2048, 1024], P(None, 'tp'), may hold values from -0.125 to 0.125
- out_weight: bfloat16 [2048, 2048], P(None, 'tp'), may hold values from -0.125 to 0.125
- chosen: int32 [96, 16], P('kv'), may hold values from 0 to 95, as said below
Outputs:
- mixed: bfloat16 [6144, 2048], P('kv', 'tp')
The draws below stay inside these ranges and needn't reach their ends.
Inputs may be any that keep to these rules, and one draw needn't show every extreme that they name: `chosen`: row b names no block after b; its first entry is b and its next 3 entries are blocks of the same device as block b; entries may repeat. Over the rows of one device, the entries after the first 4 name at most 2 blocks, counting repeats, of any one other device, and some device names exactly 2 of another.
All inputs are finite; a program needn't handle non-finite values.
Results may differ from the reference program's by a relative error of at most 0.0072.
Values may be sent and summed in bfloat16 or wider, within the bound.
A program may use at most 128 MiB of HBM per device.

```python
import jax
import jax.numpy as jnp
from jax import lax

D = 2048
H = 16
KVH = 8
HD = 128
BLK = 64
TOPB = 16
LOCAL = 3
CAP = 2
TOK_DEV = 384
TOKENS = 6144
NQB = 96
N_KV = 16


def draw_tokens(key, part):
    plain = jnp.clip(jax.random.normal(key, (TOKENS, D), jnp.float32), -6.0, 6.0)
    return plain.astype(jnp.bfloat16)


def draw_query_weight(key, part):
    fresh = jax.random.normal(jax.random.fold_in(key, 11), (D, H * HD), jnp.float32)
    return jnp.clip(fresh * D ** (-0.5), -0.5, 0.5).astype(jnp.bfloat16)


def draw_key_weight(key, part):
    fresh = jax.random.normal(jax.random.fold_in(key, 12), (D, KVH * HD), jnp.float32)
    return jnp.clip(fresh * D ** (-0.5), -0.5, 0.5).astype(jnp.bfloat16)


def draw_chosen(key, part):
    blocks = TOK_DEV // BLK
    far_count = TOPB - 1 - LOCAL
    ask_count = blocks * far_count
    picked = min(ask_count // CAP, N_KV)
    streams = jax.random.split(jax.random.fold_in(key, 21), 6)
    devices = jnp.arange(N_KV, dtype=jnp.int32)
    asking = devices[:, None]
    target = devices[None, :]
    raw_score = jax.random.randint(streams[0], (N_KV, N_KV), 0, 1 << 14)
    popular = jax.random.randint(streams[1], (1, N_KV), 0, 4) == 0
    forced = (target == asking - 1) | (target == asking - N_KV // 2)
    scores = raw_score * 1024 + target
    scores = scores + jnp.where(popular, 1 << 25, 0) + jnp.where(forced, 1 << 26, 0)
    scores = jnp.where(target < asking, scores, -1 - target)
    ranked = lax.top_k(scores, picked)[1].astype(jnp.int32)
    usable = jnp.minimum(devices, picked)
    request = jnp.arange(ask_count, dtype=jnp.int32)
    owner_slot = request // CAP
    holder = jnp.take_along_axis(ranked, jnp.broadcast_to(jnp.minimum(owner_slot, picked - 1)[None, :], (N_KV, ask_count)), axis=1)
    usable_slot = owner_slot[None, :] < usable[:, None]
    hot_block = jax.random.randint(streams[2], (N_KV,), 0, blocks)
    coin_flip = jax.random.randint(streams[3], (N_KV, ask_count), 0, 2)
    any_block = jax.random.randint(streams[4], (N_KV, ask_count), 0, blocks)
    inside = jnp.where(coin_flip == 0, hot_block[holder], any_block)
    query_block = devices[:, None] * blocks + request[None, :] // far_count
    far_ids = jnp.where(usable_slot, holder * blocks + inside, query_block).reshape(N_KV, blocks, far_count)
    own_ids = devices[:, None] * blocks + jnp.arange(blocks, dtype=jnp.int32)[None, :]
    near_raw = jax.random.randint(streams[5], (N_KV, blocks, LOCAL), 0, 1 << 16)
    near_ids = devices[:, None, None] * blocks + near_raw % (jnp.arange(blocks, dtype=jnp.int32)[None, :, None] + 1)
    table_rows = jnp.concatenate([own_ids[:, :, None], near_ids, far_ids], axis=2)
    return table_rows.reshape(N_KV * blocks, TOPB).astype(jnp.int32)


def steps_of(rng, extent, cuts, low, largest):
    loudness = 1.0
    for axis_at, blocks in cuts:
        steps = jax.random.uniform(jax.random.fold_in(jax.random.fold_in(rng, 6), axis_at), (blocks,), jnp.float32, low / len(cuts), largest / len(cuts))
        loudness = loudness * jnp.repeat(jnp.exp(steps), extent[axis_at] // blocks).reshape((-1,) + (1,) * (len(extent) - 1 - axis_at))
    return loudness


def centred(rng, dims, width, limit, cuts=(), kind=jnp.bfloat16):
    values = jax.random.normal(rng, dims, jnp.float32) * width
    if len(cuts) > 0:
        values = steps_of(rng, dims, cuts, -0.22, 0.18) * values
    return jnp.clip(values, min=-limit, max=limit).astype(kind)


def setup_inputs(seed: int = 0) -> dict:
    keys = jax.random.split(jax.random.key(seed), 7)
    return {
        "tokens": draw_tokens(jax.random.fold_in(keys[6], 71), 0),
        "query_weight": draw_query_weight(jax.random.fold_in(keys[6], 71), 0),
        "key_weight": draw_key_weight(jax.random.fold_in(keys[6], 71), 0),
        "value_weight": centred(keys[3], (D, KVH * HD), D ** -0.5, 0.125, ((1, 2),)),
        "out_weight": centred(keys[4], (H * HD, D), (H * HD) ** -0.5, 0.125, ((1, 2),)),
        "chosen": draw_chosen(jax.random.fold_in(keys[6], 71), 0),
    }


def reference(tokens, query_weight, key_weight, value_weight, out_weight, chosen):
    queries = jnp.dot(tokens, query_weight, preferred_element_type=jnp.float32).astype(jnp.bfloat16)
    key_rows = jnp.dot(tokens, key_weight, preferred_element_type=jnp.float32).astype(jnp.bfloat16)
    value_rows = jnp.dot(tokens, value_weight, preferred_element_type=jnp.float32).astype(jnp.bfloat16)
    group_size = H // KVH
    grouped = queries.reshape(NQB, BLK, KVH, group_size, HD)
    key_blocks = key_rows.reshape(NQB, BLK, KVH, HD)
    value_blocks = value_rows.reshape(NQB, BLK, KVH, HD)

    def attend(inputs):
        block_queries, chosen_row, block_number = inputs
        slot_order = jnp.arange(TOPB)
        repeats = jnp.any((chosen_row[:, None] == chosen_row[None, :]) & (slot_order[None, :] < slot_order[:, None]), axis=1)
        got_keys = jnp.take(key_blocks, chosen_row, axis=0).reshape(TOPB * BLK, KVH, HD)
        got_values = jnp.take(value_blocks, chosen_row, axis=0).reshape(TOPB * BLK, KVH, HD)
        scores = jnp.einsum("qkgd,skd->kgqs", block_queries.astype(jnp.float32), got_keys.astype(jnp.float32),
                            precision=lax.Precision.HIGHEST) * (HD ** -0.5)
        query_pos = block_number * BLK + jnp.arange(BLK, dtype=jnp.int32)
        key_pos = (chosen_row[:, None] * BLK + jnp.arange(BLK, dtype=jnp.int32)[None, :]).reshape(-1)
        fresh_slot = jnp.broadcast_to((~repeats)[:, None], (TOPB, BLK)).reshape(-1)
        visible = fresh_slot[None, :] & (key_pos[None, :] <= query_pos[:, None])
        scores = jnp.where(visible[None, None], scores, -jnp.inf)
        row_peak = jnp.max(scores, axis=-1, keepdims=True)
        weights = jnp.exp(scores - row_peak)
        row_total = jnp.sum(weights, axis=-1)
        rounded = lax.optimization_barrier(weights.astype(jnp.bfloat16)).astype(jnp.float32)
        mixed_heads = jnp.einsum("kgqs,skd->qkgd", rounded, got_values.astype(jnp.float32),
                                 precision=lax.Precision.HIGHEST)
        mixed_heads = mixed_heads / jnp.transpose(row_total, (2, 0, 1))[..., None]
        return mixed_heads.astype(jnp.bfloat16).reshape(BLK, H * HD)

    heads_out = lax.map(attend, (grouped, chosen, jnp.arange(NQB, dtype=jnp.int32)))
    return jnp.dot(heads_out.reshape(TOKENS, H * HD), out_weight, preferred_element_type=jnp.float32).astype(jnp.bfloat16)
```

```python
import functools
import math

import jax
import jax.numpy as jnp
from jax import lax
from jax.experimental import pallas as pl
from jax.experimental.pallas import tpu as pltpu
from jax.sharding import PartitionSpec as P

HD = 128
BLK = 64
CAP = 2
PLANE = 4
LOW = -1e30
SCALE = HD ** (-0.5)
VMEM = pltpu.MemorySpace.VMEM
SMEM = pltpu.MemorySpace.SMEM
NT = (((1,), (1,)), ((), ()))
TN = (((0,), (0,)), ((), ()))


def attention_kernel(
    plane, layers, lanes,
    asks_ref, bias_ref, own_bias_ref, tokens_any, wq_any, wk_any, wv_any,
    out_ref,
    held, qb, picked, stage, up_o, up_s, down_o, down_s, st_o, st_s, fr_o, fr_s,
    asked, asked_s, biasv, w_all, parts,
    w_sem, token_sem, token_send, token_recv, tell_send, tell_recv, bias_send, bias_recv, move_sem,
    climb_send, climb_recv, query_send, query_recv, side_send, side_recv, lift_send, lift_recv,
):
    heads, own_blocks = held.shape[1], held.shape[2]
    tok_rows = own_blocks * BLK
    rows = qb.shape[2]
    group = rows // tok_rows
    shares, _, depth = parts.shape
    cands = plane * CAP
    me = lax.axis_index("kv")
    core = lax.axis_index("tp")
    layer = me // plane
    seat = me % plane
    climbs = core % 2 == 0
    sinks = core % 2 == 1
    above = layer + 1 < layers
    below = layer > 0
    top = layers - 1 - layer

    def at(device, lane=None):
        return {
            "device_id": {"kv": device, "tp": core if lane is None else lane},
            "device_id_type": pl.DeviceIdType.MESH,
        }

    def peer(m):
        return layer * plane + (seat ^ m)

    def weight_copies(i):
        c = i % heads
        wide = group * HD
        kv = [
            pltpu.make_async_copy(
                wk_any.at[:, pl.ds(pl.multiple_of(c * HD, HD), HD)], w_all.at[i, :, 0:HD], w_sem.at[i, 0]
            ),
            pltpu.make_async_copy(
                wv_any.at[:, pl.ds(pl.multiple_of(c * HD, HD), HD)], w_all.at[i, :, HD:2 * HD], w_sem.at[i, 1]
            ),
        ]
        q = [
            pltpu.make_async_copy(
                wq_any.at[:, pl.ds(pl.multiple_of(c * wide, HD), wide)], w_all.at[i], w_sem.at[i, 0]
            )
        ]
        return kv, q

    def is_kv(i):
        return ((i < heads) & climbs) | ((i >= heads) & sinks)

    own_tokens = pltpu.make_async_copy(tokens_any, parts.at[0], token_sem)
    own_tokens.start()
    for i in range(2 * heads):
        kv, q = weight_copies(i)

        @pl.when(is_kv(i))
        def _():
            for copy in kv:
                copy.start()

        @pl.when(jnp.logical_not(is_kv(i)))
        def _():
            for copy in q:
                copy.start()

    asked[...] = jnp.zeros_like(asked)
    asked[0, 0] = asks_ref[...]
    biasv[0] = bias_ref[0]

    @pl.when(climbs)
    def _():
        for d in range(1, layers):
            biasv[d] = bias_ref[d]

    barrier = pltpu.get_barrier_semaphore()
    for s in range(1, shares):
        pl.semaphore_signal(barrier, inc=1, **at(me, (core + s) % shares))

    @pl.when(climbs)
    def _():
        for m in range(1, plane):
            pl.semaphore_signal(barrier, inc=1, **at(peer(m)))

        @pl.when(above)
        def _():
            pl.semaphore_signal(barrier, inc=1, **at(me + plane))

        @pl.when(below)
        def _():
            pl.semaphore_signal(barrier, inc=1, **at(me - plane))

    everyone = layers * plane

    @pl.when(sinks)
    def _():
        def greet(off, _):
            pl.semaphore_signal(barrier, inc=1, **at((me + off) % everyone))
            return 0

        lax.fori_loop(1, everyone, greet, 0)

    @pl.when(climbs)
    def _():
        pl.semaphore_wait(barrier, shares - 1 + plane - 1 + above.astype(jnp.int32) + below.astype(jnp.int32))

    @pl.when(sinks)
    def _():
        pl.semaphore_wait(barrier, shares - 1 + everyone - 1)

    def share(s):
        return pltpu.make_async_remote_copy(
            src_ref=tokens_any, dst_ref=parts.at[s], send_sem=token_send.at[s], recv_sem=token_recv.at[s],
            **at(me, (core + shares - s) % shares),
        )

    for s in range(1, shares):
        share(s).start()

    def tell(d, m):
        return pltpu.make_async_remote_copy(
            src_ref=asks_ref, dst_ref=asked.at[d, m], send_sem=tell_send.at[d, m], recv_sem=tell_recv.at[d, m],
            **at((layer - d) * plane + (seat ^ m)),
        )

    def tell_bias(d):
        return pltpu.make_async_remote_copy(
            src_ref=bias_ref.at[d], dst_ref=biasv.at[d], send_sem=bias_send.at[d], recv_sem=bias_recv.at[d],
            **at(me - d * plane),
        )

    def each_tell(far, near_act, far_act, bias_act):
        for m in range(1, plane):
            near_act(0, m)
        for d in range(1, layers):
            @pl.when(sinks & far(d))
            def _():
                for m in range(plane):
                    far_act(d, m)
                bias_act(d)

    each_tell(
        lambda d: d <= layer,
        lambda d, m: tell(d, m).start(), lambda d, m: tell(d, m).start(), lambda d: tell_bias(d).start(),
    )

    def climb(d, c):
        return pltpu.make_async_remote_copy(
            src_ref=held.at[d, c], dst_ref=held.at[d + 1, c],
            send_sem=climb_send.at[d, c], recv_sem=climb_recv.at[d + 1, c], **at(me + plane),
        )

    def sink(d, c):
        return pltpu.make_async_remote_copy(
            src_ref=qb.at[d, c], dst_ref=qb.at[d + 1, c],
            send_sem=query_send.at[d, c], recv_sem=query_recv.at[d + 1, c], **at(me - plane),
        )

    def lift(d, c):
        return [
            pltpu.make_async_remote_copy(
                src_ref=up.at[d, c], dst_ref=down.at[d - 1, c],
                send_sem=lift_send.at[d, c, n], recv_sem=lift_recv.at[d - 1, c, n], **at(me + plane),
            )
            for n, (up, down) in enumerate(((up_o, down_o), (up_s, down_s)))
        ]

    def side(d, c, m):
        return pltpu.make_async_remote_copy(
            src_ref=stage.at[d, c, m - 1], dst_ref=picked.at[d, c, m * CAP:(m + 1) * CAP],
            send_sem=side_send.at[d, c, m - 1], recv_sem=side_recv.at[d, c, m - 1], **at(peer(m)),
        )

    own_tokens.wait()
    for s in range(1, shares):
        share(s).wait_recv()

    def project(i, _):
        kv, q = weight_copies(i)
        mine = is_kv(i)
        c = i % heads

        @pl.when(mine)
        def _():
            for copy in kv:
                copy.wait()

        @pl.when(jnp.logical_not(mine))
        def _():
            for copy in q:
                copy.wait()

        total = None
        for s in range(shares):
            owner = (core + s) % shares
            term = jnp.dot(
                parts[s], w_all[i, pl.ds(pl.multiple_of(owner * depth, depth), depth), :],
                preferred_element_type=jnp.float32,
            )
            total = term if total is None else total + term
        total = total.astype(jnp.bfloat16)

        @pl.when(mine)
        def _():
            held[0, c] = total.reshape(own_blocks, BLK, 2 * HD)

            @pl.when(climbs & above)
            def _():
                climb(0, c).start()

        @pl.when(jnp.logical_not(mine))
        def _():
            for g in range(group):
                qb[0, c, g * tok_rows:(g + 1) * tok_rows] = total[:, g * HD:(g + 1) * HD]

            @pl.when(sinks & below & (top == 0))
            def _():
                sink(0, c).start()

        return 0

    lax.fori_loop(0, 2 * heads, project, 0)

    each_tell(
        lambda d: d <= top,
        lambda d, m: tell(d, m).wait_recv(), lambda d, m: tell(d, m).wait_recv(), lambda d: tell_bias(d).wait_recv(),
    )
    move = pltpu.make_async_copy(asked, asked_s, move_sem)
    move.start()
    move.wait()

    def attend(c, where_q, keys, values, mask):
        for g in range(group):
            span = slice(g * tok_rows, (g + 1) * tok_rows)
            s = lax.dot_general(keys, qb[where_q, c, span], NT, preferred_element_type=jnp.float32)
            s = mask(s.reshape(-1, BLK, tok_rows))
            peak = jnp.max(jnp.max(s, axis=0), axis=0, keepdims=True)
            p = jnp.exp((s - peak[None]) * SCALE)
            total = jnp.sum(jnp.sum(p, axis=0), axis=0, keepdims=True)
            p = p.astype(jnp.bfloat16).reshape(-1, tok_rows)
            fr_o[:, span] = lax.dot_general(values, p, TN, preferred_element_type=jnp.float32)
            fr_s[0:1, span] = peak
            fr_s[1:2, span] = total

    def merge(o_a, s_a, o_b, s_b):
        peak = jnp.maximum(s_a[0:1], s_b[0:1])
        fac_a = jnp.exp((s_a[0:1] - peak) * SCALE)
        fac_b = jnp.exp((s_b[0:1] - peak) * SCALE)
        total = s_a[1:2] * fac_a + s_b[1:2] * fac_b
        return o_a.astype(jnp.float32) * fac_a + o_b * fac_b, peak, total

    def put(o_ref, s_ref, value):
        o, peak, total = value
        o_ref[...] = o.astype(o_ref.dtype)
        s_ref[0:1] = peak
        s_ref[1:2] = total

    def local(c):
        key_at = lax.broadcasted_iota(jnp.int32, (own_blocks, BLK, tok_rows), 0) * BLK + lax.broadcasted_iota(
            jnp.int32, (own_blocks, BLK, tok_rows), 1
        )
        query_at = lax.broadcasted_iota(jnp.int32, (own_blocks, BLK, tok_rows), 2)
        own_bias = own_bias_ref[0:own_blocks]

        def mask(s):
            return jnp.where(key_at > query_at, LOW, s + own_bias[:, None, :])

        attend(
            c, 0, held[0, c, :, :, 0:HD].reshape(tok_rows, HD), held[0, c, :, :, HD:2 * HD].reshape(tok_rows, HD), mask
        )
        st_o[c] = fr_o[...]
        st_s[c] = fr_s[...]

    def choose(source, c, block):
        taken = held[source, c, 0]
        for other in range(1, own_blocks):
            taken = jnp.where(block == other, held[source, c, other], taken)
        return taken

    def distribute(d, c):
        source = jnp.where(climbs, d, 0)
        table = jnp.where(climbs, 0, d)
        for m in range(1, plane):
            for place in range(CAP):
                stage[d, c, m - 1, place] = choose(source, c, asked_s[table, m, 0, (d * plane + m) * CAP + place])
            side(d, c, m).start()
        for place in range(CAP):
            picked[d, c, place] = choose(source, c, asked_s[table, 0, 0, d * plane * CAP + place])

    def receive(i, c):
        @pl.when(climbs & (i <= layer))
        def _():
            @pl.when(i >= 1)
            def _():
                climb(i - 1, c).wait_recv()

                @pl.when(above)
                def _():
                    climb(i, c).start()

            distribute(i, c)

        d = top - i

        @pl.when(sinks & (d >= 0))
        def _():
            @pl.when(below & (d >= 1))
            def _():
                sink(d - 1, c).wait_recv()
                sink(d, c).start()

            @pl.when(below & (d == 0) & (c == 0) & (top > 0))
            def _():
                for n in range(heads):
                    sink(0, n).start()

            distribute(d, c)

        @pl.when(i == 0)
        def _():
            local(c)

    def finish(c):
        for g in range(group):
            span = slice(g * tok_rows, (g + 1) * tok_rows)
            o = st_o[c, :, span] / st_s[c, 1:2, span]
            first = pl.multiple_of((c * group + g) * HD, HD)
            out_ref[:, pl.ds(first, HD)] = o.T.astype(jnp.bfloat16)

    def compute(i, c):
        d = jnp.where(climbs, i, top - i)

        @pl.when((climbs & (i <= layer)) | (sinks & (d >= 0)))
        def _():
            away = sinks & (d >= 1)

            @pl.when(away & jnp.logical_not(below))
            def _():
                sink(d - 1, c).wait_recv()

            for m in range(1, plane):
                side(d, c, m).wait_recv()
            group_bias = biasv[d]
            attend(
                c, jnp.where(climbs, 0, d),
                picked[d, c, :, :, 0:HD].reshape(cands * BLK, HD), picked[d, c, :, :, HD:2 * HD].reshape(cands * BLK, HD),
                lambda s: s + group_bias[:, None, :],
            )

            @pl.when(away)
            def _():
                @pl.when(below)
                def _():
                    for copy in lift(d + 1, c):
                        copy.wait_recv()
                    put(up_o.at[d, c], up_s.at[d, c], merge(down_o[d, c], down_s[d, c], fr_o[...], fr_s[...]))

                @pl.when(jnp.logical_not(below))
                def _():
                    up_o[d, c] = fr_o[...].astype(jnp.bfloat16)
                    up_s[d, c] = fr_s[...]

                for copy in lift(d, c):
                    copy.start()

            @pl.when(jnp.logical_not(away))
            def _():
                put(st_o.at[c], st_s.at[c], merge(st_o[c], st_s[c], fr_o[...], fr_s[...]))

                @pl.when(sinks & below)
                def _():
                    for copy in lift(1, c):
                        copy.wait_recv()
                    put(st_o.at[c], st_s.at[c], merge(down_o[0, c], down_s[0, c], st_o[c], st_s[c]))

                @pl.when(sinks | (i == layer))
                def _():
                    finish(c)

    def step(n, _):
        i = n // heads
        c = n % heads

        @pl.when(i < layers)
        def _():
            receive(i, c)

        @pl.when(i >= 1)
        def _():
            compute(i - 1, c)

        return 0

    lax.fori_loop(0, (layers + 1) * heads, step, 0)

    for s in range(1, shares):
        share(s).wait_send()
    each_tell(
        lambda d: d <= layer,
        lambda d, m: tell(d, m).wait_send(), lambda d, m: tell(d, m).wait_send(), lambda d: tell_bias(d).wait_send(),
    )

    def drain(n, _):
        d = n // heads
        c = n % heads

        @pl.when((climbs & (d <= layer)) | (sinks & (d <= top)))
        def _():
            for m in range(1, plane):
                side(d, c, m).wait_send()

            @pl.when(climbs & above)
            def _():
                climb(d, c).wait_send()

            @pl.when(sinks & below)
            def _():
                sink(d, c).wait_send()

            @pl.when(sinks & (d >= 1))
            def _():
                for copy in lift(d, c):
                    copy.wait_send()

        return 0

    lax.fori_loop(0, layers * heads, drain, 0)


def attention(asks, bias, own_bias, tokens, query_weight, key_weight, value_weight, plane, layers):
    tok_rows, depth = tokens.shape
    width, query_cols = query_weight.shape
    cols = key_weight.shape[1]
    heads = cols // HD
    group = query_cols // cols
    rows = group * tok_rows
    own_blocks = tok_rows // BLK
    shares = width // depth
    peers = plane - 1
    lanes = asks.shape[1]
    kind = tokens.dtype
    dma = pltpu.SemaphoreType.DMA
    return pl.pallas_call(
        functools.partial(attention_kernel, plane, layers, lanes),
        out_shape=jax.ShapeDtypeStruct((tok_rows, query_cols), kind),
        in_specs=[pl.BlockSpec(memory_space=VMEM)] * 3 + [pl.BlockSpec(memory_space=pl.ANY)] * 4,
        out_specs=pl.BlockSpec(memory_space=VMEM),
        scratch_shapes=[
            pltpu.VMEM((layers, heads, own_blocks, BLK, 2 * HD), kind),
            pltpu.VMEM((layers, heads, rows, HD), kind),
            pltpu.VMEM((layers, heads, plane * CAP, BLK, 2 * HD), kind),
            pltpu.VMEM((layers, heads, peers, CAP, BLK, 2 * HD), kind),
            pltpu.VMEM((layers, heads, HD, rows), kind),
            pltpu.VMEM((layers, heads, 2, rows), jnp.float32),
            pltpu.VMEM((layers, heads, HD, rows), kind),
            pltpu.VMEM((layers, heads, 2, rows), jnp.float32),
            pltpu.VMEM((heads, HD, rows), jnp.float32),
            pltpu.VMEM((heads, 2, rows), jnp.float32),
            pltpu.VMEM((HD, rows), jnp.float32),
            pltpu.VMEM((2, rows), jnp.float32),
            pltpu.VMEM((layers, plane, 1, lanes), jnp.int32),
            pltpu.SMEM((layers, plane, 1, lanes), jnp.int32),
            pltpu.VMEM(bias.shape, jnp.float32),
            pltpu.VMEM((2 * heads, width, group * HD), kind),
            pltpu.VMEM((shares, tok_rows, depth), kind),
            dma((2 * heads, 2)), dma(()), dma((shares,)), dma((shares,)),
            dma((layers, plane)), dma((layers, plane)), dma((layers,)), dma((layers,)), dma(()),
            dma((layers, heads)), dma((layers, heads)), dma((layers, heads)), dma((layers, heads)),
            dma((layers, heads, peers)), dma((layers, heads, peers)),
            dma((layers, heads, 2)), dma((layers, heads, 2)),
        ],
        compiler_params=pltpu.CompilerParams(
            collective_id=0, has_side_effects=True, vmem_limit_bytes=60 * 2**20
        ),
    )(asks, bias, own_bias, tokens, query_weight, key_weight, value_weight)


def turned(x, shift):
    size = lax.axis_size("tp")
    return lax.ppermute(x, "tp", [((i + shift) % size, i) for i in range(size)])


def shares_of(x):
    size = lax.axis_size("tp")
    me = lax.axis_index("tp")
    return [(x if s == 0 else turned(x, s), (me + s) % size) for s in range(size)]


def tables(chosen, plane, layers):
    own_blocks = chosen.shape[0]
    device = lax.axis_index("kv")
    layer = lax.div(device, jnp.int32(plane))
    seat = device - layer * plane
    holder = lax.div(chosen, jnp.int32(own_blocks))
    within = chosen - holder * own_blocks
    holder_layer = lax.div(holder, jnp.int32(plane))
    owner = (layer - holder_layer) * plane + ((holder - holder_layer * plane) ^ seat)
    count = layers * plane
    ids = jnp.arange(count, dtype=jnp.int32)
    hit = owner.reshape(1, -1) == ids[:, None]
    low = jnp.min(jnp.where(hit, within.reshape(1, -1), own_blocks), axis=1)
    high = jnp.max(jnp.where(hit, within.reshape(1, -1), -1), axis=1)
    asks = jnp.stack([jnp.where(low < own_blocks, low, 0), jnp.maximum(high, 0)], axis=1).reshape(1, -1)
    lanes = -(-asks.shape[1] // 128) * 128
    asks = jnp.pad(asks, ((0, 0), (0, lanes - asks.shape[1])))
    far = ids >= 1
    names = jnp.stack(
        [
            jnp.where(far & (low < own_blocks), ids * own_blocks + low, -1),
            jnp.where(far & (high > low), ids * own_blocks + high, -1),
        ],
        axis=1,
    ).reshape(-1)
    names = jnp.concatenate([names, jnp.arange(8, dtype=jnp.int32)])
    wanted = jnp.repeat(jnp.transpose(owner * own_blocks + within), BLK, axis=1)
    seen = jnp.any(wanted[None] == names[:, None, None], axis=1)
    bias = jnp.where(seen, 0.0, LOW).astype(jnp.float32)
    cut = count * CAP
    return asks, bias[:cut].reshape(layers, plane * CAP, -1), bias[cut:]


def local(tokens, query_weight, key_weight, value_weight, out_weight, chosen):
    key_devices = lax.axis_size("kv")
    plane = math.gcd(key_devices, PLANE)
    layers = key_devices // plane
    asks, bias, own_bias = tables(chosen, plane, layers)
    heads_out = attention(asks, bias, own_bias, tokens, query_weight, key_weight, value_weight, plane, layers)
    (own_heads, seat), *others = shares_of(heads_out)
    first = seat * own_heads.shape[1]
    own_rows = lax.dynamic_slice_in_dim(out_weight, first, own_heads.shape[1], axis=0)
    result = jnp.dot(own_heads, own_rows, preferred_element_type=jnp.float32)
    for block, owner in others:
        result, block = lax.optimization_barrier((result, block))
        rows_of = lax.dynamic_slice_in_dim(out_weight, owner * block.shape[1], block.shape[1], axis=0)
        result = result + jnp.dot(block, rows_of, preferred_element_type=jnp.float32)
    return result.astype(jnp.bfloat16)


def solution(mesh):
    return jax.shard_map(
        local,
        mesh=mesh,
        in_specs=(
            P("kv", "tp"),
            P(None, "tp"),
            P(None, "tp"),
            P(None, "tp"),
            P(None, "tp"),
            P("kv", None),
        ),
        out_specs=P("kv", "tp"),
        check_vma=False,
    )
```

```python
import functools
import math

import jax
import jax.numpy as jnp
from jax import lax
from jax.experimental import pallas as pl
from jax.experimental.pallas import tpu as pltpu
from jax.sharding import PartitionSpec as P

HD = 128
BLK = 64
CAP = 2
PLANE = 4
LOW = -1e30
SCALE = HD ** (-0.5) * math.log2(math.e)
VMEM = pltpu.MemorySpace.VMEM
SMEM = pltpu.MemorySpace.SMEM
NT = (((1,), (1,)), ((), ()))
TN = (((0,), (0,)), ((), ()))


def attention_kernel(
    plane, layers, shares,
    asks_ref, bias_ref, own_bias_ref, wq_any, wk_any, wv_any, *refs,
):
    parts_any = refs[:shares]
    (
        out_ref,
        held, qb, picked, stage, up_o, up_s, down_o, down_s, st_o, st_s, fr_o, fr_s,
        asked, asked_s, biasv, w_all, parts,
        w_sem, token_sem, tell_send, tell_recv, bias_send, bias_recv, move_sem,
        climb_send, climb_recv, query_send, query_recv, side_send, side_recv, lift_send, lift_recv,
    ) = refs[shares:]
    heads, own_blocks = held.shape[1], held.shape[2]
    tok_rows = own_blocks * BLK
    rows = qb.shape[2]
    group = rows // tok_rows
    depth = parts.shape[2]
    cands = plane * CAP
    me = lax.axis_index("kv")
    core = lax.axis_index("tp")
    layer = me // plane
    seat = me % plane
    climbs = core % 2 == 0
    sinks = core % 2 == 1
    above = layer + 1 < layers
    below = layer > 0
    top = layers - 1 - layer
    early = min(2, heads) if layers > 2 else 0
    sent = jnp.where(layer == 1, early, 0)
    bottom = sinks & jnp.logical_not(below) & (top > 0)

    def at(device, lane=None):
        return {
            "device_id": {"kv": device, "tp": core if lane is None else lane},
            "device_id_type": pl.DeviceIdType.MESH,
        }

    def peer(m):
        return layer * plane + (seat ^ m)

    def weight_copies(i):
        c = i % heads
        wide = group * HD
        kv = [
            pltpu.make_async_copy(
                wk_any.at[:, pl.ds(pl.multiple_of(c * HD, HD), HD)], w_all.at[i, :, 0:HD], w_sem.at[i, 0]
            ),
            pltpu.make_async_copy(
                wv_any.at[:, pl.ds(pl.multiple_of(c * HD, HD), HD)], w_all.at[i, :, HD:2 * HD], w_sem.at[i, 1]
            ),
        ]
        q = [
            pltpu.make_async_copy(
                wq_any.at[:, pl.ds(pl.multiple_of(c * wide, HD), wide)], w_all.at[i], w_sem.at[i, 0]
            )
        ]
        return kv, q

    def is_kv(i):
        return ((i < heads) & climbs) | ((i >= heads) & sinks)

    token_copies = [pltpu.make_async_copy(part, parts.at[s], token_sem.at[s]) for s, part in enumerate(parts_any)]
    for copy in token_copies:
        copy.start()

    def fetch(i):
        kv, q = weight_copies(i)

        @pl.when(is_kv(i))
        def _():
            for copy in kv:
                copy.start()

        @pl.when(jnp.logical_not(is_kv(i)))
        def _():
            for copy in q:
                copy.start()

    ahead = min(3, 2 * heads)
    for i in range(ahead):
        fetch(i)

    asked[...] = jnp.zeros_like(asked)
    asked[0, 0] = asks_ref[...]
    biasv[0] = bias_ref[0]

    @pl.when(climbs)
    def _():
        for d in range(1, layers):
            biasv[d] = bias_ref[d]

    barrier = pltpu.get_barrier_semaphore()
    @pl.when(climbs)
    def _():
        for m in range(1, plane):
            pl.semaphore_signal(barrier, inc=1, **at(peer(m)))

        @pl.when(above)
        def _():
            pl.semaphore_signal(barrier, inc=1, **at(me + plane))

        @pl.when(below)
        def _():
            pl.semaphore_signal(barrier, inc=1, **at(me - plane))

    everyone = layers * plane

    @pl.when(sinks)
    def _():
        def greet(off, _):
            pl.semaphore_signal(barrier, inc=1, **at((me + off) % everyone))
            return 0

        lax.fori_loop(1, everyone, greet, 0)

    def tell(d, m):
        return pltpu.make_async_remote_copy(
            src_ref=asks_ref, dst_ref=asked.at[d, m], send_sem=tell_send.at[d, m], recv_sem=tell_recv.at[d, m],
            **at((layer - d) * plane + (seat ^ m)),
        )

    def tell_bias(d):
        return pltpu.make_async_remote_copy(
            src_ref=bias_ref.at[d], dst_ref=biasv.at[d], send_sem=bias_send.at[d], recv_sem=bias_recv.at[d],
            **at(me - d * plane),
        )

    def each_tell(far, near_act, far_act, bias_act):
        for m in range(1, plane):
            near_act(0, m)
        for d in range(1, layers):
            @pl.when(sinks & far(d))
            def _():
                for m in range(plane):
                    far_act(d, m)
                bias_act(d)

    def climb(d, c):
        return pltpu.make_async_remote_copy(
            src_ref=held.at[d, c], dst_ref=held.at[d + 1, c],
            send_sem=climb_send.at[d, c], recv_sem=climb_recv.at[d + 1, c], **at(me + plane),
        )

    def sink(d, c):
        return pltpu.make_async_remote_copy(
            src_ref=qb.at[d, c], dst_ref=qb.at[d + 1, c],
            send_sem=query_send.at[d, c], recv_sem=query_recv.at[d + 1, c], **at(me - plane),
        )

    def lift(d, c):
        return [
            pltpu.make_async_remote_copy(
                src_ref=up.at[d, c], dst_ref=down.at[d - 1, c],
                send_sem=lift_send.at[d, c, n], recv_sem=lift_recv.at[d - 1, c, n], **at(me + plane),
            )
            for n, (up, down) in enumerate(((up_o, down_o), (up_s, down_s)))
        ]

    def side(d, c, m):
        return pltpu.make_async_remote_copy(
            src_ref=stage.at[d, c, m - 1], dst_ref=picked.at[d, c, m * CAP:(m + 1) * CAP],
            send_sem=side_send.at[d, c, m - 1], recv_sem=side_recv.at[d, c, m - 1], **at(peer(m)),
        )

    def project(i):
        kv, q = weight_copies(i)
        mine = is_kv(i)
        c = i % heads

        @pl.when(mine)
        def _():
            for copy in kv:
                copy.wait()

        @pl.when(jnp.logical_not(mine))
        def _():
            for copy in q:
                copy.wait()

        @pl.when(i + ahead < 2 * heads)
        def _():
            fetch(i + ahead)

        total = None
        for s in range(shares):
            owner = (core + s) % shares
            term = jnp.dot(
                parts[s], w_all[i, pl.ds(pl.multiple_of(owner * depth, depth), depth), :],
                preferred_element_type=jnp.float32,
            )
            total = term if total is None else total + term
        total = total.astype(jnp.bfloat16)

        @pl.when(mine)
        def _():
            held[0, c] = total.reshape(own_blocks, BLK, 2 * HD)

        @pl.when(jnp.logical_not(mine))
        def _():
            for g in range(group):
                qb[0, c, g * tok_rows:(g + 1) * tok_rows] = total[:, g * HD:(g + 1) * HD]

    def launch(c):
        @pl.when(climbs & above)
        def _():
            climb(0, c).start()

        @pl.when(sinks & below & ((top == 0) | (c < sent)))
        def _():
            sink(0, c).start()

    for copy in token_copies:
        copy.wait()
    project(0)

    @pl.when(climbs)
    def _():
        pl.semaphore_wait(barrier, plane - 1 + above.astype(jnp.int32) + below.astype(jnp.int32))

    @pl.when(sinks)
    def _():
        pl.semaphore_wait(barrier, everyone - 1)

    each_tell(
        lambda d: d <= layer,
        lambda d, m: tell(d, m).start(), lambda d, m: tell(d, m).start(), lambda d: tell_bias(d).start(),
    )
    launch(0)

    def first_half(i, _):
        project(i)
        launch(i)
        return 0

    lax.fori_loop(1, heads, first_half, 0)

    def second_half(i, _):
        project(i)
        return 0

    lax.fori_loop(heads, 2 * heads, second_half, 0)
    each_tell(
        lambda d: d <= top,
        lambda d, m: tell(d, m).wait_recv(), lambda d, m: tell(d, m).wait_recv(), lambda d: tell_bias(d).wait_recv(),
    )
    move = pltpu.make_async_copy(asked, asked_s, move_sem)
    move.start()
    move.wait()

    def attend(c, where_q, keys, values, mask):
        spans = [slice(g * tok_rows, (g + 1) * tok_rows) for g in range(group)]
        raw = [lax.dot_general(keys, qb[where_q, c, span], NT, preferred_element_type=jnp.float32) for span in spans]
        rounded = []
        for span, s in zip(spans, raw):
            s = mask(s.reshape(-1, BLK, tok_rows))
            peak = jnp.max(jnp.max(s, axis=0), axis=0, keepdims=True)
            p = jnp.exp2((s - peak[None]) * SCALE)
            fr_s[0:1, span] = peak
            fr_s[1:2, span] = jnp.sum(jnp.sum(p, axis=0), axis=0, keepdims=True)
            rounded.append(p.astype(jnp.bfloat16).reshape(-1, tok_rows))
        for span, p in zip(spans, rounded):
            fr_o[:, span] = lax.dot_general(values, p, TN, preferred_element_type=jnp.float32)

    def merge(o_a, s_a, o_b, s_b):
        peak = jnp.maximum(s_a[0:1], s_b[0:1])
        fac_a = jnp.exp2((s_a[0:1] - peak) * SCALE)
        fac_b = jnp.exp2((s_b[0:1] - peak) * SCALE)
        total = s_a[1:2] * fac_a + s_b[1:2] * fac_b
        return o_a.astype(jnp.float32) * fac_a + o_b * fac_b, peak, total

    def put(o_ref, s_ref, value):
        o, peak, total = value
        o_ref[...] = o.astype(o_ref.dtype)
        s_ref[0:1] = peak
        s_ref[1:2] = total

    def local(c):
        key_at = lax.broadcasted_iota(jnp.int32, (own_blocks, BLK, tok_rows), 0) * BLK + lax.broadcasted_iota(
            jnp.int32, (own_blocks, BLK, tok_rows), 1
        )
        query_at = lax.broadcasted_iota(jnp.int32, (own_blocks, BLK, tok_rows), 2)
        own_bias = own_bias_ref[0:own_blocks]

        def mask(s):
            return jnp.where(key_at > query_at, LOW, s + own_bias[:, None, :])

        attend(
            c, 0, held[0, c, :, :, 0:HD].reshape(tok_rows, HD), held[0, c, :, :, HD:2 * HD].reshape(tok_rows, HD), mask
        )
        st_o[c] = fr_o[...]
        st_s[c] = fr_s[...]

    def choose(source, c, block):
        taken = held[source, c, 0]
        for other in range(1, own_blocks):
            taken = jnp.where(block == other, held[source, c, other], taken)
        return taken

    def distribute(d, c):
        source = jnp.where(climbs, d, 0)
        table = jnp.where(climbs, 0, d)
        for m in range(1, plane):
            for place in range(CAP):
                stage[d, c, m - 1, place] = choose(source, c, asked_s[table, m, 0, (d * plane + m) * CAP + place])
            side(d, c, m).start()
        for place in range(CAP):
            picked[d, c, place] = choose(source, c, asked_s[table, 0, 0, d * plane * CAP + place])

    def turn(n):
        i = n // heads
        c = n % heads
        plain = top - i, c
        pair = n < 2 * heads
        middle = jnp.where(pair, jnp.where(n % 2 == 0, top, 0), top - i + 1), jnp.where(pair, n // 2, c)
        if early == 0:
            lowest = plain
        else:
            m = n - early
            k = m - heads * (top - 2)
            paired = (k >= 0) & (k < 2 * heads)
            lowest = (
                jnp.where((m < 0) | (k >= 2 * heads), 1, jnp.where(paired, jnp.where(k % 2 == 0, 2, 0), top - m // heads)),
                jnp.where(m < 0, n, jnp.where(k >= 2 * heads, k - 2 * heads + early, jnp.where(paired, k // 2, m % heads))),
            )
        mixed = below & (top > 0)
        return tuple(
            jnp.where(mixed, one, jnp.where(bottom, two, three)) for one, two, three in zip(middle, lowest, plain)
        )

    busy = sinks & (top > 0)

    def pass_on(d, c):
        sink(d - 1, c).wait_recv()
        sink(d, c).start()

    def ready(c, _):
        @pl.when(busy | (climbs & (top == 0)))
        def _():
            d, at_head = turn(c)
            distribute(jnp.where(climbs, 0, d), jnp.where(climbs, c, at_head))

        return 0

    lax.fori_loop(0, heads, ready, 0)

    def forward(i, c):
        @pl.when(climbs & (i >= 1) & (i <= layer))
        def _():
            climb(i - 1, c).wait_recv()

            @pl.when(above)
            def _():
                climb(i, c).start()

        d = top - i

        @pl.when(sinks & below & (d >= 1))
        def _():
            pass_on(d, c)

        @pl.when(sinks & below & (d == 0) & (c == 0) & (top > 0))
        def _():
            def send(n, _):
                sink(0, n).start()
                return 0

            lax.fori_loop(sent, heads, send, 0)

    def finish(c):
        @pl.when(sinks & below)
        def _():
            for copy in lift(1, c):
                copy.wait_recv()
            put(st_o.at[c], st_s.at[c], merge(down_o[0, c], down_s[0, c], st_o[c], st_s[c]))

        for g in range(group):
            span = slice(g * tok_rows, (g + 1) * tok_rows)
            o = st_o[c, :, span] / st_s[c, 1:2, span]
            first = pl.multiple_of((c * group + g) * HD, HD)
            out_ref[:, pl.ds(first, HD)] = o.T.astype(jnp.bfloat16)

    def compute(d, c):
        away = sinks & (d >= 1)

        @pl.when(away & jnp.logical_not(below))
        def _():
            sink(d - 1, c).wait_recv()

        for m in range(1, plane):
            side(d, c, m).wait_recv()
        group_bias = biasv[d]
        attend(
            c, jnp.where(climbs, 0, d),
            picked[d, c, :, :, 0:HD].reshape(cands * BLK, HD), picked[d, c, :, :, HD:2 * HD].reshape(cands * BLK, HD),
            lambda s: s + group_bias[:, None, :],
        )

        @pl.when(away)
        def _():
            @pl.when(below)
            def _():
                for copy in lift(d + 1, c):
                    copy.wait_recv()
                put(up_o.at[d, c], up_s.at[d, c], merge(down_o[d, c], down_s[d, c], fr_o[...], fr_s[...]))

            @pl.when(jnp.logical_not(below))
            def _():
                up_o[d, c] = fr_o[...].astype(jnp.bfloat16)
                up_s[d, c] = fr_s[...]

            for copy in lift(d, c):
                copy.start()

        @pl.when(jnp.logical_not(away))
        def _():
            put(st_o.at[c], st_s.at[c], merge(st_o[c], st_s[c], fr_o[...], fr_s[...]))

    lag = jnp.where(climbs & above, 2, jnp.where(bottom, 0, 1))

    def step(n, _):
        i = n // heads
        c = n % heads

        @pl.when(i < layers)
        def _():
            forward(i, c)

        due = i - jnp.where(climbs & above, 1, 0)
        shift = jnp.where(bottom, heads, 0)

        @pl.when((climbs & (due >= jnp.where(above, 0, 1)) & (due <= layer)) | (sinks & (n + shift < (top + 1) * heads) & ((top == 0) | (i > 0) | bottom)))
        def _():
            d, at_head = turn(n + shift)
            distribute(jnp.where(climbs, due, d), jnp.where(climbs, c, at_head))

        @pl.when((i == 0) & jnp.logical_not(bottom))
        def _():
            local(c)

        @pl.when(bottom & (n == early))
        def _():
            def each(h, _):
                local(h)
                return 0

            lax.fori_loop(0, heads, each, 0)

        back = i - lag

        @pl.when((back >= 0) & ((climbs & (back <= layer)) | (sinks & (back <= top))))
        def _():
            d, at_head = turn(n - lag * heads)
            compute(jnp.where(climbs, back, d), jnp.where(climbs, c, at_head))

        return 0

    lax.fori_loop(0, (layers + 2) * heads, step, 0)

    def last(c, _):
        finish(c)
        return 0

    lax.fori_loop(0, heads, last, 0)

    each_tell(
        lambda d: d <= layer,
        lambda d, m: tell(d, m).wait_send(), lambda d, m: tell(d, m).wait_send(), lambda d: tell_bias(d).wait_send(),
    )

    def drain(n, _):
        d = n // heads
        c = n % heads

        @pl.when((climbs & (d <= layer)) | (sinks & (d <= top)))
        def _():
            for m in range(1, plane):
                side(d, c, m).wait_send()

            @pl.when(climbs & above)
            def _():
                climb(d, c).wait_send()

            @pl.when(sinks & below)
            def _():
                sink(d, c).wait_send()

            @pl.when(sinks & (d >= 1))
            def _():
                for copy in lift(d, c):
                    copy.wait_send()

        return 0

    lax.fori_loop(0, layers * heads, drain, 0)


def attention(asks, bias, own_bias, parts, query_weight, key_weight, value_weight, plane, layers):
    tok_rows, depth = parts[0].shape
    width, query_cols = query_weight.shape
    cols = key_weight.shape[1]
    heads = cols // HD
    group = query_cols // cols
    rows = group * tok_rows
    own_blocks = tok_rows // BLK
    shares = len(parts)
    peers = plane - 1
    lanes = asks.shape[1]
    kind = parts[0].dtype
    dma = pltpu.SemaphoreType.DMA
    return pl.pallas_call(
        functools.partial(attention_kernel, plane, layers, shares),
        out_shape=jax.ShapeDtypeStruct((tok_rows, query_cols), kind),
        in_specs=[pl.BlockSpec(memory_space=VMEM)] * 3 + [pl.BlockSpec(memory_space=pl.ANY)] * (3 + shares),
        out_specs=pl.BlockSpec(memory_space=VMEM),
        scratch_shapes=[
            pltpu.VMEM((layers, heads, own_blocks, BLK, 2 * HD), kind),
            pltpu.VMEM((layers, heads, rows, HD), kind),
            pltpu.VMEM((layers, heads, plane * CAP, BLK, 2 * HD), kind),
            pltpu.VMEM((layers, heads, peers, CAP, BLK, 2 * HD), kind),
            pltpu.VMEM((layers, heads, HD, rows), kind),
            pltpu.VMEM((layers, heads, 2, rows), jnp.float32),
            pltpu.VMEM((layers, heads, HD, rows), kind),
            pltpu.VMEM((layers, heads, 2, rows), jnp.float32),
            pltpu.VMEM((heads, HD, rows), jnp.float32),
            pltpu.VMEM((heads, 2, rows), jnp.float32),
            pltpu.VMEM((HD, rows), jnp.float32),
            pltpu.VMEM((2, rows), jnp.float32),
            pltpu.VMEM((layers, plane, 1, lanes), jnp.int32),
            pltpu.SMEM((layers, plane, 1, lanes), jnp.int32),
            pltpu.VMEM(bias.shape, jnp.float32),
            pltpu.VMEM((2 * heads, width, group * HD), kind),
            pltpu.VMEM((shares, tok_rows, depth), kind),
            dma((2 * heads, 2)), dma((shares,)),
            dma((layers, plane)), dma((layers, plane)), dma((layers,)), dma((layers,)), dma(()),
            dma((layers, heads)), dma((layers, heads)), dma((layers, heads)), dma((layers, heads)),
            dma((layers, heads, peers)), dma((layers, heads, peers)),
            dma((layers, heads, 2)), dma((layers, heads, 2)),
        ],
        compiler_params=pltpu.CompilerParams(
            collective_id=0, has_side_effects=True, vmem_limit_bytes=60 * 2**20
        ),
    )(asks, bias, own_bias, query_weight, key_weight, value_weight, *parts)


def turned(x, shift):
    size = lax.axis_size("tp")
    return lax.ppermute(x, "tp", [((i + shift) % size, i) for i in range(size)])


def shares_of(x):
    size = lax.axis_size("tp")
    me = lax.axis_index("tp")
    return [(x if s == 0 else turned(x, s), (me + s) % size) for s in range(size)]


def tables(chosen, plane, layers):
    own_blocks = chosen.shape[0]
    device = lax.axis_index("kv")
    layer = lax.div(device, jnp.int32(plane))
    seat = device - layer * plane
    holder = lax.div(chosen, jnp.int32(own_blocks))
    within = chosen - holder * own_blocks
    holder_layer = lax.div(holder, jnp.int32(plane))
    owner = (layer - holder_layer) * plane + ((holder - holder_layer * plane) ^ seat)
    count = layers * plane
    ids = jnp.arange(count, dtype=jnp.int32)
    hit = owner.reshape(1, -1) == ids[:, None]
    low = jnp.min(jnp.where(hit, within.reshape(1, -1), own_blocks), axis=1)
    high = jnp.max(jnp.where(hit, within.reshape(1, -1), -1), axis=1)
    asks = jnp.stack([jnp.where(low < own_blocks, low, 0), jnp.maximum(high, 0)], axis=1).reshape(1, -1)
    lanes = -(-asks.shape[1] // 128) * 128
    asks = jnp.pad(asks, ((0, 0), (0, lanes - asks.shape[1])))
    far = ids >= 1
    names = jnp.stack(
        [
            jnp.where(far & (low < own_blocks), ids * own_blocks + low, -1),
            jnp.where(far & (high > low), ids * own_blocks + high, -1),
        ],
        axis=1,
    ).reshape(-1)
    names = jnp.concatenate([names, jnp.arange(8, dtype=jnp.int32)])
    wanted = jnp.repeat(jnp.transpose(owner * own_blocks + within), BLK, axis=1)
    seen = jnp.any(wanted[None] == names[:, None, None], axis=1)
    bias = jnp.where(seen, 0.0, LOW).astype(jnp.float32)
    cut = count * CAP
    return asks, bias[:cut].reshape(layers, plane * CAP, -1), bias[cut:]


def local(tokens, query_weight, key_weight, value_weight, out_weight, chosen):
    key_devices = lax.axis_size("kv")
    plane = math.gcd(key_devices, PLANE)
    layers = key_devices // plane
    asks, bias, own_bias = tables(chosen, plane, layers)
    parts = [block for block, _ in shares_of(tokens)]
    heads_out = attention(asks, bias, own_bias, parts, query_weight, key_weight, value_weight, plane, layers)
    (own_heads, seat), *others = shares_of(heads_out)
    first = seat * own_heads.shape[1]
    own_rows = lax.dynamic_slice_in_dim(out_weight, first, own_heads.shape[1], axis=0)
    result = jnp.dot(own_heads, own_rows, preferred_element_type=jnp.float32)
    for block, owner in others:
        result, block = lax.optimization_barrier((result, block))
        rows_of = lax.dynamic_slice_in_dim(out_weight, owner * block.shape[1], block.shape[1], axis=0)
        result = result + jnp.dot(block, rows_of, preferred_element_type=jnp.float32)
    return result.astype(jnp.bfloat16)


def solution(mesh):
    return jax.shard_map(
        local,
        mesh=mesh,
        in_specs=(
            P("kv", "tp"),
            P(None, "tp"),
            P(None, "tp"),
            P(None, "tp"),
            P(None, "tp"),
            P("kv", None),
        ),
        out_specs=P("kv", "tp"),
        check_vma=False,
    )
```

```python
import functools
import math

import jax
import jax.numpy as jnp
from jax import lax
from jax.experimental import pallas as pl
from jax.experimental.pallas import tpu as pltpu
from jax.sharding import PartitionSpec as P

HD = 128
BLK = 64
CAP = 2
PLANE = 4
LOW = -1e30
SCALE = HD ** (-0.5) * math.log2(math.e)
VMEM = pltpu.MemorySpace.VMEM
SMEM = pltpu.MemorySpace.SMEM
NT = (((1,), (1,)), ((), ()))
TN = (((0,), (0,)), ((), ()))


def attention_kernel(
    plane, layers, shares,
    asks_ref, bias_ref, own_bias_ref, wq_any, wk_any, wv_any, wo_any, *refs,
):
    parts_any = refs[:shares]
    (
        out_vmem,
        held, qb, picked, stage, up_o, up_s, down_o, down_s, st_o, st_s, fr_o, fr_s,
        asked, asked_s, biasv, w_all, parts, wo, ho, acc,
        w_sem, token_sem, go_sem, tell_send, tell_recv, bias_send, bias_recv, move_sem,
        flow_send, flow_recv, side_send, side_recv, lift_send, lift_recv, wo_sem, give_send, give_recv,
    ) = refs[shares:]
    heads, own_blocks = held.shape[1], held.shape[2]
    tok_rows = own_blocks * BLK
    rows = qb.shape[2]
    group = rows // tok_rows
    depth = parts.shape[2]
    cands = plane * CAP
    me = lax.axis_index("kv")
    core = lax.axis_index("tp")
    layer = me // plane
    seat = me % plane
    climbs = core % 2 == 0
    sinks = core % 2 == 1
    above = layer + 1 < layers
    below = layer > 0
    top = layers - 1 - layer
    early = min(2, heads) if layers > 2 else 0
    sent = jnp.where(layer == 1, early, 0)
    bottom = sinks & jnp.logical_not(below) & (top > 0)

    def at(device, lane=None):
        return {
            "device_id": {"kv": device, "tp": core if lane is None else lane},
            "device_id_type": pl.DeviceIdType.MESH,
        }

    def peer(m):
        return layer * plane + (seat ^ m)

    ahead = min(3, 2 * heads)

    def weight_copies(i):
        c = i % heads
        wide = group * HD
        kv = [
            pltpu.make_async_copy(
                wk_any.at[:, pl.ds(pl.multiple_of(c * HD, HD), HD)], w_all.at[i, :, 0:HD], w_sem.at[i % ahead]
            ),
            pltpu.make_async_copy(
                wv_any.at[:, pl.ds(pl.multiple_of(c * HD, HD), HD)], w_all.at[i, :, HD:2 * HD], w_sem.at[i % ahead]
            ),
        ]
        q = [
            pltpu.make_async_copy(
                wq_any.at[:, pl.ds(pl.multiple_of(c * wide, HD), wide)], w_all.at[i], w_sem.at[i % ahead]
            )
        ]
        return kv, q

    def is_kv(i):
        return ((i < heads) & climbs) | ((i >= heads) & sinks)

    token_copies = [pltpu.make_async_copy(part, parts.at[s], token_sem.at[s]) for s, part in enumerate(parts_any)]
    for copy in token_copies:
        copy.start()

    def fetch(i):
        kv, q = weight_copies(i)

        @pl.when(is_kv(i))
        def _():
            for copy in kv:
                copy.start()

        @pl.when(jnp.logical_not(is_kv(i)))
        def _():
            for copy in q:
                copy.start()

    for i in range(ahead):
        fetch(i)

    asked[...] = jnp.zeros_like(asked)
    asked[0, 0] = asks_ref[...]
    biasv[0] = bias_ref[0]

    @pl.when(climbs)
    def _():
        for d in range(1, layers):
            biasv[d] = bias_ref[d]

    barrier = pltpu.get_barrier_semaphore()
    gated = ((top >= 2) | (top == 0)) & (core + jnp.where(climbs, 1, 0) < shares)
    mate = core + 1 - 2 * (core % 2)
    for share in range(1, shares):
        pl.semaphore_signal(barrier, inc=1, **at(me, (core + share) % shares))

    @pl.when(climbs)
    def _():
        for m in range(1, plane):
            pl.semaphore_signal(barrier, inc=1, **at(peer(m)))

        @pl.when(above)
        def _():
            pl.semaphore_signal(barrier, inc=1, **at(me + plane))

        @pl.when(below)
        def _():
            pl.semaphore_signal(barrier, inc=1, **at(me - plane))

    everyone = layers * plane

    @pl.when(sinks)
    def _():
        def greet(off, _):
            pl.semaphore_signal(barrier, inc=1, **at((me + off) % everyone))
            return 0

        lax.fori_loop(1, everyone, greet, 0)

    def tell(d, m):
        return pltpu.make_async_remote_copy(
            src_ref=asks_ref, dst_ref=asked.at[d, m], send_sem=tell_send.at[d], recv_sem=tell_recv.at[d],
            **at((layer - d) * plane + (seat ^ m)),
        )

    def tell_bias(d):
        return pltpu.make_async_remote_copy(
            src_ref=bias_ref.at[d], dst_ref=biasv.at[d], send_sem=bias_send.at[d], recv_sem=bias_recv.at[d],
            **at(me - d * plane),
        )

    def tells(d):
        first = 1 if d == 0 else 0
        span = asked.at[d, first:plane]
        return pltpu.make_async_remote_copy(
            src_ref=span, dst_ref=span, send_sem=tell_send.at[d], recv_sem=tell_recv.at[d], **at(me - d * plane)
            if d else at(peer(1)),
        )

    def each_tell(far, act, bias_act):
        act(0)
        for d in range(1, layers):
            @pl.when(sinks & far(d))
            def _():
                act(d)
                bias_act(d)

    def tell_all(d):
        for m in range(1 if d == 0 else 0, plane):
            tell(d, m).start()

    def climb(d, c):
        return pltpu.make_async_remote_copy(
            src_ref=held.at[d, c], dst_ref=held.at[d + 1, c],
            send_sem=flow_send.at[d], recv_sem=flow_recv.at[d, c], **at(me + plane),
        )

    def sink(d, c):
        return pltpu.make_async_remote_copy(
            src_ref=qb.at[d, c], dst_ref=qb.at[d + 1, c],
            send_sem=flow_send.at[d], recv_sem=flow_recv.at[d, c], **at(me - plane),
        )

    def lift(d, c):
        return [
            pltpu.make_async_remote_copy(
                src_ref=up.at[d, c], dst_ref=down.at[d - 1, c],
                send_sem=lift_send.at[d, n], recv_sem=lift_recv.at[d - 1, c, n], **at(me + plane),
            )
            for n, (up, down) in enumerate(((up_o, down_o), (up_s, down_s)))
        ]

    def side(d, c, m):
        return pltpu.make_async_remote_copy(
            src_ref=stage.at[d, c, (m - 1) * CAP:m * CAP], dst_ref=picked.at[d, c, m * CAP:(m + 1) * CAP],
            send_sem=side_send.at[d], recv_sem=side_recv.at[d, c], **at(peer(m)),
        )

    def sides(d, c):
        return pltpu.make_async_remote_copy(
            src_ref=stage.at[d, c], dst_ref=picked.at[d, c, CAP:plane * CAP],
            send_sem=side_send.at[d], recv_sem=side_recv.at[d, c], **at(peer(1)),
        )

    def project(i):
        mine = is_kv(i)
        c = i % heads

        pltpu.make_async_copy(w_all.at[i], w_all.at[i], w_sem.at[i % ahead]).wait()

        @pl.when(i + ahead < 2 * heads)
        def _():
            fetch(i + ahead)

        total = None
        for s in range(shares):
            owner = (core + s) % shares
            term = jnp.dot(
                parts[s], w_all[i, pl.ds(pl.multiple_of(owner * depth, depth), depth), :],
                preferred_element_type=jnp.float32,
            )
            total = term if total is None else total + term
        total = total.astype(jnp.bfloat16)

        @pl.when(mine)
        def _():
            held[0, c] = total.reshape(own_blocks, BLK, 2 * HD)

        @pl.when(jnp.logical_not(mine))
        def _():
            for g in range(group):
                qb[0, c, g * tok_rows:(g + 1) * tok_rows] = total[:, g * HD:(g + 1) * HD]

    def launch(c):
        @pl.when(climbs & above)
        def _():
            climb(0, c).start()

        @pl.when(sinks & below & ((top == 0) | (c < sent)))
        def _():
            sink(0, c).start()

    for copy in token_copies:
        copy.wait()
    project(0)

    @pl.when(climbs)
    def _():
        pl.semaphore_wait(barrier, plane - 1 + above.astype(jnp.int32) + below.astype(jnp.int32) + shares - 1)

    @pl.when(sinks)
    def _():
        pl.semaphore_wait(barrier, everyone + shares - 2)

    each_tell(lambda d: d <= layer, tell_all, lambda d: tell_bias(d).start())
    launch(0)

    def first_half(i, _):
        project(i)
        launch(i)
        return 0

    lax.fori_loop(1, heads, first_half, 0)

    def second_half(i, _):
        project(i)
        return 0

    lax.fori_loop(heads, 2 * heads, second_half, 0)
    fetch_out = pltpu.make_async_copy(wo_any, wo, wo_sem)
    fetch_out.start()
    acc[...] = jnp.zeros_like(acc)
    each_tell(lambda d: d <= top, lambda d: tells(d).wait_recv(), lambda d: tell_bias(d).wait_recv())
    move = pltpu.make_async_copy(asked, asked_s, move_sem)
    move.start()
    move.wait()

    def attend(c, where_q, keys, values, mask):
        spans = [slice(g * tok_rows, (g + 1) * tok_rows) for g in range(group)]
        raw = [lax.dot_general(keys, qb[where_q, c, span], NT, preferred_element_type=jnp.float32) for span in spans]
        rounded = []
        for span, s in zip(spans, raw):
            s = mask(s.reshape(-1, BLK, tok_rows))
            peak = jnp.max(jnp.max(s, axis=0), axis=0, keepdims=True)
            p = jnp.exp2((s - peak[None]) * SCALE)
            fr_s[0:1, span] = peak
            fr_s[1:2, span] = jnp.sum(jnp.sum(p, axis=0), axis=0, keepdims=True)
            rounded.append(p.astype(jnp.bfloat16).reshape(-1, tok_rows))
        for span, p in zip(spans, rounded):
            fr_o[:, span] = lax.dot_general(values, p, TN, preferred_element_type=jnp.float32)

    def merge(o_a, s_a, o_b, s_b):
        peak = jnp.maximum(s_a[0:1], s_b[0:1])
        fac_a = jnp.exp2((s_a[0:1] - peak) * SCALE)
        fac_b = jnp.exp2((s_b[0:1] - peak) * SCALE)
        total = s_a[1:2] * fac_a + s_b[1:2] * fac_b
        return o_a.astype(jnp.float32) * fac_a + o_b * fac_b, peak, total

    def put(o_ref, s_ref, value):
        o, peak, total = value
        o_ref[...] = o.astype(o_ref.dtype)
        s_ref[0:1] = peak
        s_ref[1:2] = total

    def local(c):
        key_at = lax.broadcasted_iota(jnp.int32, (own_blocks, BLK, tok_rows), 0) * BLK + lax.broadcasted_iota(
            jnp.int32, (own_blocks, BLK, tok_rows), 1
        )
        query_at = lax.broadcasted_iota(jnp.int32, (own_blocks, BLK, tok_rows), 2)
        own_bias = own_bias_ref[0:own_blocks]

        def mask(s):
            return jnp.where(key_at > query_at, LOW, s + own_bias[:, None, :])

        attend(
            c, 0, held[0, c, :, :, 0:HD].reshape(tok_rows, HD), held[0, c, :, :, HD:2 * HD].reshape(tok_rows, HD), mask
        )
        st_o[c] = fr_o[...]
        st_s[c] = fr_s[...]

    def choose(source, c, block):
        taken = held[source, c, 0]
        for other in range(1, own_blocks):
            taken = jnp.where(block == other, held[source, c, other], taken)
        return taken

    def distribute(d, c):
        source = jnp.where(climbs, d, 0)
        table = jnp.where(climbs, 0, d)
        for m in range(1, plane):
            for place in range(CAP):
                stage[d, c, (m - 1) * CAP + place] = choose(source, c, asked_s[table, m, 0, (d * plane + m) * CAP + place])
            side(d, c, m).start()
        for place in range(CAP):
            picked[d, c, place] = choose(source, c, asked_s[table, 0, 0, d * plane * CAP + place])

    def turn(n):
        i = n // heads
        own_first = below & (top == 1)
        plain = jnp.where(own_first, i, top - i), n % heads
        if early == 0:
            return plain
        moved = bottom & (n >= early) & (n < (top - 1) * heads + early)
        lead = bottom & (n < early)
        m = n - early
        return (
            jnp.where(lead, 1, jnp.where(moved, top - m // heads, plain[0])),
            jnp.where(lead, n, jnp.where(moved, m % heads, plain[1])),
        )

    busy = sinks & (top > 0)

    def pass_on(d, c):
        sink(d - 1, c).wait_recv()
        sink(d, c).start()

    def ready(c, _):
        @pl.when((busy & (c < (top + 1) * heads)) | (climbs & (top == 0) & (c < heads)))
        def _():
            d, at_head = turn(c)
            distribute(jnp.where(climbs, 0, d), jnp.where(climbs, c, at_head))

        return 0

    lax.fori_loop(0, layers * heads, ready, 0)

    def forward(i, c):
        @pl.when(climbs & (i >= 1) & (i <= layer))
        def _():
            climb(i - 1, c).wait_recv()

            @pl.when(above)
            def _():
                climb(i, c).start()

        d = top - i

        @pl.when(sinks & below & (d >= 1))
        def _():
            pass_on(d, c)

        @pl.when(sinks & below & (d == 0) & (c == 0) & (top > 0))
        def _():
            def send(n, _):
                sink(0, n).start()
                return 0

            lax.fori_loop(sent, heads, send, 0)

    def finish(c):
        @pl.when(sinks & below)
        def _():
            for copy in lift(1, c):
                copy.wait_recv()
            put(st_o.at[c], st_s.at[c], merge(down_o[0, c], down_s[0, c], st_o[c], st_s[c]))

        for g in range(group):
            span = slice(g * tok_rows, (g + 1) * tok_rows)
            o = st_o[c, :, span] / st_s[c, 1:2, span]
            ho[0, c, :, g * HD:(g + 1) * HD] = o.T.astype(jnp.bfloat16)

        for share in range(1, shares):
            give(share, c).start()

    def give(share, c):
        return pltpu.make_async_remote_copy(
            src_ref=ho.at[0, c], dst_ref=ho.at[share, c],
            send_sem=give_send.at[share], recv_sem=give_recv.at[share, c], **at(me, (core + shares - share) % shares),
        )

    wide = group * HD
    out_cols = out_vmem.shape[1]
    tile = min(256, out_cols)

    def mixed_in(share, c, first):
        owner = (core + share) % shares
        rows_of = pl.multiple_of((owner * heads + c) * wide, wide)
        return jnp.dot(
            ho[share, c], wo[pl.ds(rows_of, wide), first:first + tile], preferred_element_type=jnp.float32
        )

    def compute(d, c):
        away = sinks & (d >= 1)

        @pl.when(away & jnp.logical_not(below))
        def _():
            sink(d - 1, c).wait_recv()

        sides(d, c).wait_recv()
        group_bias = biasv[d]
        attend(
            c, jnp.where(climbs, 0, d),
            picked[d, c, :, :, 0:HD].reshape(cands * BLK, HD), picked[d, c, :, :, HD:2 * HD].reshape(cands * BLK, HD),
            lambda s: s + group_bias[:, None, :],
        )

        @pl.when(away)
        def _():
            @pl.when(below)
            def _():
                for copy in lift(d + 1, c):
                    copy.wait_recv()
                put(up_o.at[d, c], up_s.at[d, c], merge(down_o[d, c], down_s[d, c], fr_o[...], fr_s[...]))

            @pl.when(jnp.logical_not(below))
            def _():
                up_o[d, c] = fr_o[...].astype(jnp.bfloat16)
                up_s[d, c] = fr_s[...]

            for copy in lift(d, c):
                copy.start()

        @pl.when(jnp.logical_not(away))
        def _():
            put(st_o.at[c], st_s.at[c], merge(st_o[c], st_s[c], fr_o[...], fr_s[...]))

    hold = jnp.where(climbs, jnp.where(top >= 2, 2, jnp.where(above, 1, 0)), jnp.where((top == 0) & below, 1, 0))
    lag = jnp.where(bottom, 0, hold + 1)

    def step(n, _):
        i = n // heads
        c = n % heads

        @pl.when(i < layers)
        def _():
            forward(i, c)

        due = i - hold

        waits = gated & (climbs ^ (top == 0))

        @pl.when(waits & (n == hold * heads))
        def _():
            pl.semaphore_wait(go_sem, 1)

        @pl.when(gated & jnp.logical_not(waits) & (n == jnp.where(climbs, 2 * heads, jnp.where(below, 1, heads))))
        def _():
            pl.semaphore_signal(go_sem, inc=1, **at(me, mate))

        first_due = jnp.where(above, 0, 1)

        @pl.when((climbs & (due >= first_due) & (due <= layer)) | (sinks & (top == 0) & (due == 0)))
        def _():
            distribute(due, c)

        @pl.when((i == 0) & jnp.logical_not(bottom))
        def _():
            local(c)

        @pl.when(bottom & (n == early))
        def _():
            def each(h, _):
                local(h)
                return 0

            lax.fori_loop(0, heads, each, 0)

        back = i - lag

        @pl.when((back >= 0) & ((climbs & (back <= layer)) | (sinks & (back <= top))))
        def _():
            d, at_head = turn(n - lag * heads)
            compute(jnp.where(climbs, back, d), jnp.where(climbs, c, at_head))

        return 0

    lax.fori_loop(0, (layers + 3) * heads, step, 0)

    def last(c, _):
        finish(c)
        for first in range(0, out_cols, tile):
            acc[:, first:first + tile] += mixed_in(0, c, first)

        return 0

    fetch_out.wait()
    lax.fori_loop(0, heads, last, 0)

    def other(n, _):
        share = 1 + n // heads
        c = n % heads
        give(share, c).wait_recv()
        for first in range(0, out_cols, tile):
            acc[:, first:first + tile] += mixed_in(share, c, first)
        return 0

    total = (shares - 1) * heads
    lax.fori_loop(0, total - 1, other, 0)
    for share in range(max(shares - 1, 1), shares):
        give(share, heads - 1).wait_recv()
    for first in range(0, out_cols, tile):
        value = acc[:, first:first + tile]
        for share in range(max(shares - 1, 1), shares):
            value = value + mixed_in(share, heads - 1, first)
        out_vmem[:, first:first + tile] = value.astype(jnp.bfloat16)

    each_tell(lambda d: d <= layer, lambda d: tells(d).wait_send(), lambda d: tell_bias(d).wait_send())

    def sent_all(ref, sem):
        return pltpu.make_async_remote_copy(src_ref=ref, dst_ref=ref, send_sem=sem, recv_sem=sem, **at(peer(1)))

    def drain(d, _):
        @pl.when((climbs & (d <= layer)) | (sinks & (d <= top)))
        def _():
            sent_all(stage.at[d], side_send.at[d]).wait_send()

            @pl.when(climbs & above)
            def _():
                sent_all(held.at[d], flow_send.at[d]).wait_send()

            @pl.when(sinks & below)
            def _():
                sent_all(qb.at[d], flow_send.at[d]).wait_send()

            @pl.when(sinks & (d >= 1))
            def _():
                sent_all(up_o.at[d], lift_send.at[d, 0]).wait_send()
                sent_all(up_s.at[d], lift_send.at[d, 1]).wait_send()

        return 0

    lax.fori_loop(0, layers, drain, 0)
    for share in range(1, shares):
        sent_all(ho.at[0], give_send.at[share]).wait_send()


def attention(asks, bias, own_bias, parts, query_weight, key_weight, value_weight, out_weight, plane, layers):
    tok_rows, depth = parts[0].shape
    width, query_cols = query_weight.shape
    cols = key_weight.shape[1]
    heads = cols // HD
    group = query_cols // cols
    rows = group * tok_rows
    own_blocks = tok_rows // BLK
    out_cols = out_weight.shape[1]
    shares = len(parts)
    peers = plane - 1
    lanes = asks.shape[1]
    kind = parts[0].dtype
    dma = pltpu.SemaphoreType.DMA
    return pl.pallas_call(
        functools.partial(attention_kernel, plane, layers, shares),
        out_shape=jax.ShapeDtypeStruct((tok_rows, out_cols), kind),
        in_specs=[pl.BlockSpec(memory_space=VMEM)] * 3 + [pl.BlockSpec(memory_space=pl.ANY)] * (4 + shares),
        out_specs=pl.BlockSpec(memory_space=VMEM),
        scratch_shapes=[
            pltpu.VMEM((layers, heads, own_blocks, BLK, 2 * HD), kind),
            pltpu.VMEM((layers, heads, rows, HD), kind),
            pltpu.VMEM((layers, heads, plane * CAP, BLK, 2 * HD), kind),
            pltpu.VMEM((layers, heads, peers * CAP, BLK, 2 * HD), kind),
            pltpu.VMEM((layers, heads, HD, rows), kind),
            pltpu.VMEM((layers, heads, 2, rows), jnp.float32),
            pltpu.VMEM((layers, heads, HD, rows), kind),
            pltpu.VMEM((layers, heads, 2, rows), jnp.float32),
            pltpu.VMEM((heads, HD, rows), jnp.float32),
            pltpu.VMEM((heads, 2, rows), jnp.float32),
            pltpu.VMEM((HD, rows), jnp.float32),
            pltpu.VMEM((2, rows), jnp.float32),
            pltpu.VMEM((layers, plane, 1, lanes), jnp.int32),
            pltpu.SMEM((layers, plane, 1, lanes), jnp.int32),
            pltpu.VMEM(bias.shape, jnp.float32),
            pltpu.VMEM((2 * heads, width, group * HD), kind),
            pltpu.VMEM((shares, tok_rows, depth), kind),
            pltpu.VMEM(out_weight.shape, kind),
            pltpu.VMEM((shares, heads, tok_rows, group * HD), kind),
            pltpu.VMEM((tok_rows, out_cols), jnp.float32),
            dma((min(3, 2 * heads),)), dma((shares,)), pltpu.SemaphoreType.REGULAR,
            dma((layers,)), dma((layers,)), dma((layers,)), dma((layers,)), dma(()),
            dma((layers,)), dma((layers, heads)), dma((layers,)), dma((layers, heads)),
            dma((layers, 2)), dma((layers, heads, 2)),
            dma(()), dma((shares,)), dma((shares, heads)),
        ],
        compiler_params=pltpu.CompilerParams(
            collective_id=0, has_side_effects=True, vmem_limit_bytes=52 * 2**20
        ),
    )(asks, bias, own_bias, query_weight, key_weight, value_weight, out_weight, *parts)


def turned(x, shift):
    size = lax.axis_size("tp")
    return lax.ppermute(x, "tp", [((i + shift) % size, i) for i in range(size)])


def shares_of(x):
    size = lax.axis_size("tp")
    me = lax.axis_index("tp")
    return [(x if s == 0 else turned(x, s), (me + s) % size) for s in range(size)]


def tables(chosen, plane, layers):
    own_blocks = chosen.shape[0]
    device = lax.axis_index("kv")
    layer = lax.div(device, jnp.int32(plane))
    seat = device - layer * plane
    holder = lax.div(chosen, jnp.int32(own_blocks))
    within = chosen - holder * own_blocks
    holder_layer = lax.div(holder, jnp.int32(plane))
    owner = (layer - holder_layer) * plane + ((holder - holder_layer * plane) ^ seat)
    count = layers * plane
    ids = jnp.arange(count, dtype=jnp.int32)
    hit = owner.reshape(1, -1) == ids[:, None]
    low = jnp.min(jnp.where(hit, within.reshape(1, -1), own_blocks), axis=1)
    high = jnp.max(jnp.where(hit, within.reshape(1, -1), -1), axis=1)
    asks = jnp.stack([jnp.where(low < own_blocks, low, 0), jnp.maximum(high, 0)], axis=1).reshape(1, -1)
    lanes = -(-asks.shape[1] // 128) * 128
    asks = jnp.pad(asks, ((0, 0), (0, lanes - asks.shape[1])))
    far = ids >= 1
    names = jnp.stack(
        [
            jnp.where(far & (low < own_blocks), ids * own_blocks + low, -1),
            jnp.where(far & (high > low), ids * own_blocks + high, -1),
        ],
        axis=1,
    ).reshape(-1)
    names = jnp.concatenate([names, jnp.arange(8, dtype=jnp.int32)])
    wanted = jnp.repeat(jnp.transpose(owner * own_blocks + within), BLK, axis=1)
    seen = jnp.any(wanted[None] == names[:, None, None], axis=1)
    bias = jnp.where(seen, 0.0, LOW).astype(jnp.float32)
    cut = count * CAP
    return asks, bias[:cut].reshape(layers, plane * CAP, -1), bias[cut:]


def local(tokens, query_weight, key_weight, value_weight, out_weight, chosen):
    key_devices = lax.axis_size("kv")
    plane = math.gcd(key_devices, PLANE)
    layers = key_devices // plane
    asks, bias, own_bias = tables(chosen, plane, layers)
    parts = [block for block, _ in shares_of(tokens)]
    return attention(
        asks, bias, own_bias, parts, query_weight, key_weight, value_weight, out_weight, plane, layers
    )


def solution(mesh):
    return jax.shard_map(
        local,
        mesh=mesh,
        in_specs=(
            P("kv", "tp"),
            P(None, "tp"),
            P(None, "tp"),
            P(None, "tp"),
            P(None, "tp"),
            P("kv", None),
        ),
        out_specs=P("kv", "tp"),
        check_vma=False,
    )
```

```python
import functools
import math

import jax
import jax.numpy as jnp
from jax import lax
from jax.experimental import pallas as pl
from jax.experimental.pallas import tpu as pltpu
from jax.sharding import PartitionSpec as P

HD = 128
BLK = 64
CAP = 2
PLANE = 4
LOW = -1e30
SCALE = HD ** (-0.5) * math.log2(math.e)
VMEM = pltpu.MemorySpace.VMEM
SMEM = pltpu.MemorySpace.SMEM
NT = (((1,), (1,)), ((), ()))
TN = (((0,), (0,)), ((), ()))


def attention_kernel(
    plane, layers, shares,
    asks_ref, bias_ref, own_bias_ref, wq_any, wk_any, wv_any, wo_any, *refs,
):
    parts_any = refs[:shares]
    (
        out_vmem,
        held, qb, picked, stage, up_o, up_s, down_o, down_s, st_o, st_s, fr_o, fr_s,
        asked, asked_s, biasv, w_all, parts, wo, ho, acc,
        w_sem, token_sem, go_sem, tell_send, tell_recv, bias_send, bias_recv, move_sem,
        flow_send, flow_recv, side_send, side_recv, lift_send, lift_recv, wo_sem, give_send, give_recv,
    ) = refs[shares:]
    heads, own_blocks = held.shape[1], held.shape[2]
    tok_rows = own_blocks * BLK
    rows = qb.shape[2]
    group = rows // tok_rows
    depth = parts.shape[2]
    cands = plane * CAP
    me = lax.axis_index("kv")
    core = lax.axis_index("tp")
    layer = me // plane
    seat = me % plane
    climbs = core % 2 == 0
    sinks = core % 2 == 1
    above = layer + 1 < layers
    below = layer > 0
    top = layers - 1 - layer
    early = min(2, heads) if layers > 2 else 0
    sent = jnp.where(layer == 1, early, 0)
    bottom = sinks & jnp.logical_not(below) & (top > 0)

    def at(device, lane=None):
        return {
            "device_id": {"kv": device, "tp": core if lane is None else lane},
            "device_id_type": pl.DeviceIdType.MESH,
        }

    def peer(m):
        return layer * plane + (seat ^ m)

    ahead = min(3, 2 * heads)

    def weight_copies(i):
        c = i % heads
        wide = group * HD
        kv = [
            pltpu.make_async_copy(
                wk_any.at[:, pl.ds(pl.multiple_of(c * HD, HD), HD)], w_all.at[i, :, 0:HD], w_sem.at[i % ahead]
            ),
            pltpu.make_async_copy(
                wv_any.at[:, pl.ds(pl.multiple_of(c * HD, HD), HD)], w_all.at[i, :, HD:2 * HD], w_sem.at[i % ahead]
            ),
        ]
        q = [
            pltpu.make_async_copy(
                wq_any.at[:, pl.ds(pl.multiple_of(c * wide, HD), wide)], w_all.at[i], w_sem.at[i % ahead]
            )
        ]
        return kv, q

    def is_kv(i):
        return ((i < heads) & climbs) | ((i >= heads) & sinks)

    token_copies = [pltpu.make_async_copy(part, parts.at[s], token_sem.at[s]) for s, part in enumerate(parts_any)]
    for copy in token_copies:
        copy.start()

    def fetch(i):
        kv, q = weight_copies(i)

        @pl.when(is_kv(i))
        def _():
            for copy in kv:
                copy.start()

        @pl.when(jnp.logical_not(is_kv(i)))
        def _():
            for copy in q:
                copy.start()

    for i in range(ahead):
        fetch(i)

    asked[...] = jnp.zeros_like(asked)
    asked[0, 0] = asks_ref[...]
    biasv[0] = bias_ref[0]

    @pl.when(climbs)
    def _():
        for d in range(1, layers):
            biasv[d] = bias_ref[d]

    barrier = pltpu.get_barrier_semaphore()
    gated = ((top >= 2) | (top == 0)) & (core + jnp.where(climbs, 1, 0) < shares)
    mate = core + 1 - 2 * (core % 2)
    for share in range(1, shares):
        pl.semaphore_signal(barrier, inc=1, **at(me, (core + share) % shares))

    for m in range(1, plane):
        pl.semaphore_signal(barrier, inc=1, **at(peer(m)))

    @pl.when(below)
    def _():
        pl.semaphore_signal(barrier, inc=1, **at(me - plane))

    @pl.when(sinks)
    def _():
        def greet(device, _):
            pl.semaphore_signal(barrier, inc=1, **at(device))
            return 0

        lax.fori_loop((layer + 1) * plane, layers * plane, greet, 0)

    def tell(d, m):
        return pltpu.make_async_remote_copy(
            src_ref=asks_ref, dst_ref=asked.at[d, m], send_sem=tell_send.at[d], recv_sem=tell_recv.at[d],
            **at((layer - d) * plane + (seat ^ m)),
        )

    def tell_bias(d):
        return pltpu.make_async_remote_copy(
            src_ref=bias_ref.at[d], dst_ref=biasv.at[d], send_sem=bias_send.at[d], recv_sem=bias_recv.at[d],
            **at(me - d * plane),
        )

    def tells(d):
        first = 1 if d == 0 else 0
        span = asked.at[d, first:plane]
        return pltpu.make_async_remote_copy(
            src_ref=span, dst_ref=span, send_sem=tell_send.at[d], recv_sem=tell_recv.at[d], **at(me - d * plane)
            if d else at(peer(1)),
        )

    def each_tell(far, act, bias_act):
        act(0)
        for d in range(1, layers):
            @pl.when(sinks & far(d))
            def _():
                act(d)
                bias_act(d)

    def tell_all(d):
        for m in range(1 if d == 0 else 0, plane):
            tell(d, m).start()

    def climb(d, c):
        return pltpu.make_async_remote_copy(
            src_ref=held.at[d, c], dst_ref=held.at[d + 1, c],
            send_sem=flow_send.at[d], recv_sem=flow_recv.at[d, c], **at(me + plane),
        )

    def sink(d, c):
        return pltpu.make_async_remote_copy(
            src_ref=qb.at[d, c], dst_ref=qb.at[d + 1, c],
            send_sem=flow_send.at[d], recv_sem=flow_recv.at[d, c], **at(me - plane),
        )

    def lift(d, c):
        return [
            pltpu.make_async_remote_copy(
                src_ref=up.at[d, c], dst_ref=down.at[d - 1, c],
                send_sem=lift_send.at[d, n], recv_sem=lift_recv.at[d - 1, c, n], **at(me + plane),
            )
            for n, (up, down) in enumerate(((up_o, down_o), (up_s, down_s)))
        ]

    def side(d, c, m):
        return pltpu.make_async_remote_copy(
            src_ref=stage.at[d, c, (m - 1) * CAP:m * CAP], dst_ref=picked.at[d, c, m * CAP:(m + 1) * CAP],
            send_sem=side_send.at[d], recv_sem=side_recv.at[d, c], **at(peer(m)),
        )

    def sides(d, c):
        return pltpu.make_async_remote_copy(
            src_ref=stage.at[d, c], dst_ref=picked.at[d, c, CAP:plane * CAP],
            send_sem=side_send.at[d], recv_sem=side_recv.at[d, c], **at(peer(1)),
        )

    def project(i):
        mine = is_kv(i)
        c = i % heads

        pltpu.make_async_copy(w_all.at[i], w_all.at[i], w_sem.at[i % ahead]).wait()

        @pl.when(i + ahead < 2 * heads)
        def _():
            fetch(i + ahead)

        total = None
        for s in range(shares):
            owner = (core + s) % shares
            term = jnp.dot(
                parts[s], w_all[i, pl.ds(pl.multiple_of(owner * depth, depth), depth), :],
                preferred_element_type=jnp.float32,
            )
            total = term if total is None else total + term
        total = total.astype(jnp.bfloat16)

        @pl.when(mine)
        def _():
            held[0, c] = total.reshape(own_blocks, BLK, 2 * HD)

        @pl.when(jnp.logical_not(mine))
        def _():
            for g in range(group):
                qb[0, c, g * tok_rows:(g + 1) * tok_rows] = total[:, g * HD:(g + 1) * HD]

    def launch(c):
        @pl.when(climbs & above)
        def _():
            climb(0, c).start()

        @pl.when(sinks & below & ((top == 0) | (c < sent)))
        def _():
            sink(0, c).start()

    for copy in token_copies:
        copy.wait()
    project(0)

    pl.semaphore_wait(barrier, shares + plane - 2 + above.astype(jnp.int32) + jnp.where(sinks, layer * plane, 0))
    each_tell(lambda d: d <= layer, tell_all, lambda d: tell_bias(d).start())
    launch(0)

    def first_half(i, _):
        project(i)
        launch(i)
        return 0

    lax.fori_loop(1, heads, first_half, 0)

    def second_half(i, _):
        project(i)
        return 0

    lax.fori_loop(heads, 2 * heads, second_half, 0)
    fetch_out = pltpu.make_async_copy(wo_any, wo, wo_sem)
    fetch_out.start()
    acc[...] = jnp.zeros_like(acc)
    each_tell(lambda d: d <= top, lambda d: tells(d).wait_recv(), lambda d: tell_bias(d).wait_recv())
    move = pltpu.make_async_copy(asked, asked_s, move_sem)
    move.start()
    move.wait()

    def attend(c, where_q, keys, values, mask):
        spans = [slice(g * tok_rows, (g + 1) * tok_rows) for g in range(group)]
        raw = [lax.dot_general(keys, qb[where_q, c, span], NT, preferred_element_type=jnp.float32) for span in spans]
        rounded = []
        for span, s in zip(spans, raw):
            s = mask(s.reshape(-1, BLK, tok_rows))
            peak = jnp.max(jnp.max(s, axis=0), axis=0, keepdims=True)
            p = jnp.exp2((s - peak[None]) * SCALE)
            fr_s[0:1, span] = peak
            fr_s[1:2, span] = jnp.sum(jnp.sum(p, axis=0), axis=0, keepdims=True)
            rounded.append(p.astype(jnp.bfloat16).reshape(-1, tok_rows))
        for span, p in zip(spans, rounded):
            fr_o[:, span] = lax.dot_general(values, p, TN, preferred_element_type=jnp.float32)

    def merge(o_a, s_a, o_b, s_b):
        peak = jnp.maximum(s_a[0:1], s_b[0:1])
        fac_a = jnp.exp2((s_a[0:1] - peak) * SCALE)
        fac_b = jnp.exp2((s_b[0:1] - peak) * SCALE)
        total = s_a[1:2] * fac_a + s_b[1:2] * fac_b
        return o_a.astype(jnp.float32) * fac_a + o_b * fac_b, peak, total

    def put(o_ref, s_ref, value):
        o, peak, total = value
        o_ref[...] = o.astype(o_ref.dtype)
        s_ref[0:1] = peak
        s_ref[1:2] = total

    def local(c):
        key_at = lax.broadcasted_iota(jnp.int32, (own_blocks, BLK, tok_rows), 0) * BLK + lax.broadcasted_iota(
            jnp.int32, (own_blocks, BLK, tok_rows), 1
        )
        query_at = lax.broadcasted_iota(jnp.int32, (own_blocks, BLK, tok_rows), 2)
        own_bias = own_bias_ref[0:own_blocks]

        def mask(s):
            return jnp.where(key_at > query_at, LOW, s + own_bias[:, None, :])

        attend(
            c, 0, held[0, c, :, :, 0:HD].reshape(tok_rows, HD), held[0, c, :, :, HD:2 * HD].reshape(tok_rows, HD), mask
        )
        st_o[c] = fr_o[...]
        st_s[c] = fr_s[...]

    def choose(source, c, block):
        taken = held[source, c, 0]
        for other in range(1, own_blocks):
            taken = jnp.where(block == other, held[source, c, other], taken)
        return taken

    def distribute(d, c):
        source = jnp.where(climbs, d, 0)
        table = jnp.where(climbs, 0, d)
        for m in range(1, plane):
            for place in range(CAP):
                stage[d, c, (m - 1) * CAP + place] = choose(source, c, asked_s[table, m, 0, (d * plane + m) * CAP + place])
            side(d, c, m).start()
        for place in range(CAP):
            picked[d, c, place] = choose(source, c, asked_s[table, 0, 0, d * plane * CAP + place])

    def turn(n):
        i = n // heads
        c = n % heads
        k = n - heads * (top - 1)
        paired = (k >= 0) & below & (top > 1)
        d = jnp.where(below & (top == 1), i, top - i)
        d = jnp.where(paired, jnp.where(k % 2 == 0, 1, 0), d)
        c = jnp.where(paired, k // 2, c)
        if early > 0:
            m = n - early
            k = m - heads * (top - 2)
            low = jnp.where(k % 2 == 0, 2, 0)
            low = jnp.where((m < 0) | (k >= 2 * heads), 1, jnp.where(k >= 0, low, top - m // heads))
            at_low = jnp.where(k >= 2 * heads, k - 2 * heads + early, jnp.where(k >= 0, k // 2, m % heads))
            d = jnp.where(bottom, low, d)
            c = jnp.where(bottom, jnp.where(m < 0, n, at_low), c)
        return d, c

    busy = sinks & (top > 0)

    def pass_on(d, c):
        sink(d - 1, c).wait_recv()
        sink(d, c).start()

    def ready(c, _):
        @pl.when((busy & (c < (top + 1) * heads)) | (climbs & (top == 0) & (c < heads)))
        def _():
            d, at_head = turn(c)
            distribute(jnp.where(climbs, 0, d), jnp.where(climbs, c, at_head))

        return 0

    lax.fori_loop(0, layers * heads, ready, 0)

    def forward(i, c):
        @pl.when(climbs & (i >= 1) & (i <= layer))
        def _():
            climb(i - 1, c).wait_recv()

            @pl.when(above)
            def _():
                climb(i, c).start()

        d = top - i

        @pl.when(sinks & below & (d >= 1))
        def _():
            pass_on(d, c)

        @pl.when(sinks & below & (d == 0) & (c == 0) & (top > 0))
        def _():
            def send(n, _):
                sink(0, n).start()
                return 0

            lax.fori_loop(sent, heads, send, 0)

    def finish(c):
        @pl.when(sinks & below)
        def _():
            for copy in lift(1, c):
                copy.wait_recv()
            put(st_o.at[c], st_s.at[c], merge(down_o[0, c], down_s[0, c], st_o[c], st_s[c]))

        for g in range(group):
            span = slice(g * tok_rows, (g + 1) * tok_rows)
            o = st_o[c, :, span] / st_s[c, 1:2, span]
            ho[0, c, :, g * HD:(g + 1) * HD] = o.T.astype(jnp.bfloat16)

        for share in range(1, shares):
            give(share, c).start()

    def give(share, c):
        return pltpu.make_async_remote_copy(
            src_ref=ho.at[0, c], dst_ref=ho.at[share, c],
            send_sem=give_send.at[share], recv_sem=give_recv.at[share, c], **at(me, (core + shares - share) % shares),
        )

    wide = group * HD
    out_cols = out_vmem.shape[1]
    tile = min(256, out_cols)

    def mixed_in(share, c, first):
        owner = (core + share) % shares
        rows_of = pl.multiple_of((owner * heads + c) * wide, wide)
        return jnp.dot(
            ho[share, c], wo[pl.ds(rows_of, wide), first:first + tile], preferred_element_type=jnp.float32
        )

    def compute(d, c):
        away = sinks & (d >= 1)

        @pl.when(away & jnp.logical_not(below))
        def _():
            sink(d - 1, c).wait_recv()

        sides(d, c).wait_recv()
        group_bias = biasv[d]
        attend(
            c, jnp.where(climbs, 0, d),
            picked[d, c, :, :, 0:HD].reshape(cands * BLK, HD), picked[d, c, :, :, HD:2 * HD].reshape(cands * BLK, HD),
            lambda s: s + group_bias[:, None, :],
        )

        @pl.when(away)
        def _():
            @pl.when(below)
            def _():
                for copy in lift(d + 1, c):
                    copy.wait_recv()
                put(up_o.at[d, c], up_s.at[d, c], merge(down_o[d, c], down_s[d, c], fr_o[...], fr_s[...]))

            @pl.when(jnp.logical_not(below))
            def _():
                up_o[d, c] = fr_o[...].astype(jnp.bfloat16)
                up_s[d, c] = fr_s[...]

            for copy in lift(d, c):
                copy.start()

        @pl.when(jnp.logical_not(away))
        def _():
            put(st_o.at[c], st_s.at[c], merge(st_o[c], st_s[c], fr_o[...], fr_s[...]))

    hold = jnp.where(climbs, jnp.where(top >= 2, 2, jnp.where(above, 1, 0)), jnp.where((top == 0) & below, 1, 0))
    lag = jnp.where(bottom, 0, hold + 1)

    def step(n, _):
        i = n // heads
        c = n % heads

        @pl.when(i < layers)
        def _():
            forward(i, c)

        due = i - hold

        waits = gated & (climbs ^ (top == 0))

        @pl.when(waits & (n == hold * heads))
        def _():
            pl.semaphore_wait(go_sem, 1)

        @pl.when(gated & jnp.logical_not(waits) & (n == jnp.where(climbs, 3 * heads - 2, jnp.where(below, 1, heads))))
        def _():
            pl.semaphore_signal(go_sem, inc=1, **at(me, mate))

        first_due = jnp.where(above, 0, 1)

        @pl.when((climbs & (due >= first_due) & (due <= layer)) | (sinks & (top == 0) & (due == 0)))
        def _():
            distribute(due, c)

        @pl.when((i == 0) & jnp.logical_not(bottom))
        def _():
            local(c)

        @pl.when(bottom & (n == early))
        def _():
            def each(h, _):
                local(h)
                return 0

            lax.fori_loop(0, heads, each, 0)

        back = i - lag

        @pl.when((back >= 0) & ((climbs & (back <= layer)) | (sinks & (back <= top))))
        def _():
            d, at_head = turn(n - lag * heads)
            compute(jnp.where(climbs, back, d), jnp.where(climbs, c, at_head))

        return 0

    lax.fori_loop(0, (layers + 3) * heads, step, 0)

    def last(c, _):
        finish(c)
        for first in range(0, out_cols, tile):
            acc[:, first:first + tile] += mixed_in(0, c, first)

        return 0

    fetch_out.wait()
    lax.fori_loop(0, heads, last, 0)

    def other(n, _):
        share = 1 + n // heads
        c = n % heads
        give(share, c).wait_recv()
        for first in range(0, out_cols, tile):
            acc[:, first:first + tile] += mixed_in(share, c, first)
        return 0

    total = (shares - 1) * heads
    lax.fori_loop(0, total - 1, other, 0)
    for share in range(max(shares - 1, 1), shares):
        give(share, heads - 1).wait_recv()
    for first in range(0, out_cols, tile):
        value = acc[:, first:first + tile]
        for share in range(max(shares - 1, 1), shares):
            value = value + mixed_in(share, heads - 1, first)
        out_vmem[:, first:first + tile] = value.astype(jnp.bfloat16)

    each_tell(lambda d: d <= layer, lambda d: tells(d).wait_send(), lambda d: tell_bias(d).wait_send())

    def sent_all(ref, sem):
        return pltpu.make_async_remote_copy(src_ref=ref, dst_ref=ref, send_sem=sem, recv_sem=sem, **at(peer(1)))

    def drain(d, _):
        @pl.when((climbs & (d <= layer)) | (sinks & (d <= top)))
        def _():
            sent_all(stage.at[d], side_send.at[d]).wait_send()

            @pl.when(climbs & above)
            def _():
                sent_all(held.at[d], flow_send.at[d]).wait_send()

            @pl.when(sinks & below)
            def _():
                sent_all(qb.at[d], flow_send.at[d]).wait_send()

            @pl.when(sinks & (d >= 1))
            def _():
                sent_all(up_o.at[d], lift_send.at[d, 0]).wait_send()
                sent_all(up_s.at[d], lift_send.at[d, 1]).wait_send()

        return 0

    lax.fori_loop(0, layers, drain, 0)
    for share in range(1, shares):
        sent_all(ho.at[0], give_send.at[share]).wait_send()


def attention(asks, bias, own_bias, parts, query_weight, key_weight, value_weight, out_weight, plane, layers):
    tok_rows, depth = parts[0].shape
    width, query_cols = query_weight.shape
    cols = key_weight.shape[1]
    heads = cols // HD
    group = query_cols // cols
    rows = group * tok_rows
    own_blocks = tok_rows // BLK
    out_cols = out_weight.shape[1]
    shares = len(parts)
    peers = plane - 1
    lanes = asks.shape[1]
    kind = parts[0].dtype
    dma = pltpu.SemaphoreType.DMA
    return pl.pallas_call(
        functools.partial(attention_kernel, plane, layers, shares),
        out_shape=jax.ShapeDtypeStruct((tok_rows, out_cols), kind),
        in_specs=[pl.BlockSpec(memory_space=VMEM)] * 3 + [pl.BlockSpec(memory_space=pl.ANY)] * (4 + shares),
        out_specs=pl.BlockSpec(memory_space=VMEM),
        scratch_shapes=[
            pltpu.VMEM((layers, heads, own_blocks, BLK, 2 * HD), kind),
            pltpu.VMEM((layers, heads, rows, HD), kind),
            pltpu.VMEM((layers, heads, plane * CAP, BLK, 2 * HD), kind),
            pltpu.VMEM((layers, heads, peers * CAP, BLK, 2 * HD), kind),
            pltpu.VMEM((layers, heads, HD, rows), kind),
            pltpu.VMEM((layers, heads, 2, rows), jnp.float32),
            pltpu.VMEM((layers, heads, HD, rows), kind),
            pltpu.VMEM((layers, heads, 2, rows), jnp.float32),
            pltpu.VMEM((heads, HD, rows), jnp.float32),
            pltpu.VMEM((heads, 2, rows), jnp.float32),
            pltpu.VMEM((HD, rows), jnp.float32),
            pltpu.VMEM((2, rows), jnp.float32),
            pltpu.VMEM((layers, plane, 1, lanes), jnp.int32),
            pltpu.SMEM((layers, plane, 1, lanes), jnp.int32),
            pltpu.VMEM(bias.shape, jnp.float32),
            pltpu.VMEM((2 * heads, width, group * HD), kind),
            pltpu.VMEM((shares, tok_rows, depth), kind),
            pltpu.VMEM(out_weight.shape, kind),
            pltpu.VMEM((shares, heads, tok_rows, group * HD), kind),
            pltpu.VMEM((tok_rows, out_cols), jnp.float32),
            dma((min(3, 2 * heads),)), dma((shares,)), pltpu.SemaphoreType.REGULAR,
            dma((layers,)), dma((layers,)), dma((layers,)), dma((layers,)), dma(()),
            dma((layers,)), dma((layers, heads)), dma((layers,)), dma((layers, heads)),
            dma((layers, 2)), dma((layers, heads, 2)),
            dma(()), dma((shares,)), dma((shares, heads)),
        ],
        compiler_params=pltpu.CompilerParams(
            collective_id=0, has_side_effects=True, vmem_limit_bytes=53 * 2**20
        ),
    )(asks, bias, own_bias, query_weight, key_weight, value_weight, out_weight, *parts)


def turned(x, shift):
    size = lax.axis_size("tp")
    return lax.ppermute(x, "tp", [((i + shift) % size, i) for i in range(size)])


def shares_of(x):
    size = lax.axis_size("tp")
    me = lax.axis_index("tp")
    return [(x if s == 0 else turned(x, s), (me + s) % size) for s in range(size)]


def tables(chosen, plane, layers):
    own_blocks = chosen.shape[0]
    device = lax.axis_index("kv")
    layer = lax.div(device, jnp.int32(plane))
    seat = device - layer * plane
    holder = lax.div(chosen, jnp.int32(own_blocks))
    within = chosen - holder * own_blocks
    holder_layer = lax.div(holder, jnp.int32(plane))
    owner = (layer - holder_layer) * plane + ((holder - holder_layer * plane) ^ seat)
    count = layers * plane
    ids = jnp.arange(count, dtype=jnp.int32)
    hit = owner.reshape(1, -1) == ids[:, None]
    low = jnp.min(jnp.where(hit, within.reshape(1, -1), own_blocks), axis=1)
    high = jnp.max(jnp.where(hit, within.reshape(1, -1), -1), axis=1)
    asks = jnp.stack([jnp.where(low < own_blocks, low, 0), jnp.maximum(high, 0)], axis=1).reshape(1, -1)
    lanes = -(-asks.shape[1] // 128) * 128
    asks = jnp.pad(asks, ((0, 0), (0, lanes - asks.shape[1])))
    far = ids >= 1
    names = jnp.stack(
        [
            jnp.where(far & (low < own_blocks), ids * own_blocks + low, -1),
            jnp.where(far & (high > low), ids * own_blocks + high, -1),
        ],
        axis=1,
    ).reshape(-1)
    names = jnp.concatenate([names, jnp.arange(8, dtype=jnp.int32)])
    wanted = jnp.repeat(jnp.transpose(owner * own_blocks + within), BLK, axis=1)
    seen = jnp.any(wanted[None] == names[:, None, None], axis=1)
    bias = jnp.where(seen, 0.0, LOW).astype(jnp.float32)
    cut = count * CAP
    return asks, bias[:cut].reshape(layers, plane * CAP, -1), bias[cut:]


def local(tokens, query_weight, key_weight, value_weight, out_weight, chosen):
    key_devices = lax.axis_size("kv")
    plane = math.gcd(key_devices, PLANE)
    layers = key_devices // plane
    asks, bias, own_bias = tables(chosen, plane, layers)
    parts = [block for block, _ in shares_of(tokens)]
    return attention(
        asks, bias, own_bias, parts, query_weight, key_weight, value_weight, out_weight, plane, layers
    )


def solution(mesh):
    return jax.shard_map(
        local,
        mesh=mesh,
        in_specs=(
            P("kv", "tp"),
            P(None, "tp"),
            P(None, "tp"),
            P(None, "tp"),
            P(None, "tp"),
            P("kv", None),
        ),
        out_specs=P("kv", "tp"),
        check_vma=False,
    )
```

```python
import functools
import math

import jax
import jax.numpy as jnp
from jax import lax
from jax.experimental import pallas as pl
from jax.experimental.pallas import tpu as pltpu
from jax.sharding import PartitionSpec as P

HD = 128
BLK = 64
CAP = 2
PLANE = 4
LOW = -1e30
SCALE = HD ** (-0.5) * math.log2(math.e)
VMEM = pltpu.MemorySpace.VMEM
SMEM = pltpu.MemorySpace.SMEM
NT = (((1,), (1,)), ((), ()))
TN = (((0,), (0,)), ((), ()))


def attention_kernel(
    plane, layers, shares,
    asks_ref, bias_ref, own_bias_ref, wq_any, wk_any, wv_any, wo_any, *refs,
):
    parts_any = refs[:shares]
    (
        out_vmem,
        held, qb, picked, stage, up_o, up_s, down_o, down_s, st_o, st_s, fr_o, fr_s,
        asked, asked_s, biasv, w_all, parts, wo, ho, acc,
        w_sem, token_sem, go_sem, tell_send, tell_recv, bias_send, bias_recv, move_sem,
        flow_send, flow_recv, side_send, side_recv, lift_send, lift_recv, wo_sem, give_send, give_recv,
    ) = refs[shares:]
    heads, own_blocks = held.shape[1], held.shape[2]
    tok_rows = own_blocks * BLK
    rows = qb.shape[2]
    group = rows // tok_rows
    depth = parts.shape[2]
    cands = plane * CAP
    me = lax.axis_index("kv")
    core = lax.axis_index("tp")
    layer = me // plane
    seat = me % plane
    climbs = core % 2 == 0
    sinks = core % 2 == 1
    above = layer + 1 < layers
    below = layer > 0
    top = layers - 1 - layer
    early = min(2, heads) if layers > 2 else 0
    sent = jnp.where(layer == 1, early, 0)
    bottom = sinks & jnp.logical_not(below) & (top > 0)
    spread = bottom & (layers >= plane)

    def at(device, lane=None):
        return {
            "device_id": {"kv": device, "tp": core if lane is None else lane},
            "device_id_type": pl.DeviceIdType.MESH,
        }

    def peer(m):
        return layer * plane + (seat ^ m)

    ahead = min(3, 2 * heads)

    def weight_copies(i):
        c = i % heads
        wide = group * HD
        kv = [
            pltpu.make_async_copy(
                wk_any.at[:, pl.ds(pl.multiple_of(c * HD, HD), HD)], w_all.at[i, :, 0:HD], w_sem.at[i % ahead]
            ),
            pltpu.make_async_copy(
                wv_any.at[:, pl.ds(pl.multiple_of(c * HD, HD), HD)], w_all.at[i, :, HD:2 * HD], w_sem.at[i % ahead]
            ),
        ]
        q = [
            pltpu.make_async_copy(
                wq_any.at[:, pl.ds(pl.multiple_of(c * wide, HD), wide)], w_all.at[i], w_sem.at[i % ahead]
            )
        ]
        return kv, q

    def is_kv(i):
        keys_first = climbs | spread
        return ((i < heads) & keys_first) | ((i >= heads) & jnp.logical_not(keys_first))

    token_copies = [pltpu.make_async_copy(part, parts.at[s], token_sem.at[s]) for s, part in enumerate(parts_any)]
    for copy in token_copies:
        copy.start()

    def fetch(i):
        kv, q = weight_copies(i)

        @pl.when(is_kv(i))
        def _():
            for copy in kv:
                copy.start()

        @pl.when(jnp.logical_not(is_kv(i)))
        def _():
            for copy in q:
                copy.start()

    for i in range(ahead):
        fetch(i)

    asked[...] = jnp.zeros_like(asked)
    asked[0, 0] = asks_ref[...]
    biasv[0] = bias_ref[0]

    @pl.when(climbs)
    def _():
        for d in range(1, layers):
            biasv[d] = bias_ref[d]

    barrier = pltpu.get_barrier_semaphore()
    gated = ((top >= 2) | (top == 0)) & (core + jnp.where(climbs, 1, 0) < shares)
    mate = core + 1 - 2 * (core % 2)
    for share in range(1, shares):
        pl.semaphore_signal(barrier, inc=1, **at(me, (core + share) % shares))

    for m in range(1, plane):
        pl.semaphore_signal(barrier, inc=1, **at(peer(m)))

    @pl.when(below)
    def _():
        pl.semaphore_signal(barrier, inc=1, **at(me - plane))

    @pl.when(sinks)
    def _():
        def greet(device, _):
            pl.semaphore_signal(barrier, inc=1, **at(device))
            return 0

        lax.fori_loop((layer + 1) * plane, layers * plane, greet, 0)

    def tell(d, m):
        return pltpu.make_async_remote_copy(
            src_ref=asks_ref, dst_ref=asked.at[d, m], send_sem=tell_send.at[d], recv_sem=tell_recv.at[d],
            **at((layer - d) * plane + (seat ^ m)),
        )

    def tell_bias(d):
        return pltpu.make_async_remote_copy(
            src_ref=bias_ref.at[d], dst_ref=biasv.at[d], send_sem=bias_send.at[d], recv_sem=bias_recv.at[d],
            **at(me - d * plane),
        )

    def tells(d):
        first = 1 if d == 0 else 0
        span = asked.at[d, first:plane]
        return pltpu.make_async_remote_copy(
            src_ref=span, dst_ref=span, send_sem=tell_send.at[d], recv_sem=tell_recv.at[d], **at(me - d * plane)
            if d else at(peer(1)),
        )

    def each_tell(far, act, bias_act):
        act(0)
        for d in range(1, layers):
            @pl.when(sinks & far(d))
            def _():
                act(d)
                bias_act(d)

    def tell_all(d):
        for m in range(1 if d == 0 else 0, plane):
            tell(d, m).start()

    def climb(d, c):
        return pltpu.make_async_remote_copy(
            src_ref=held.at[d, c], dst_ref=held.at[d + 1, c],
            send_sem=flow_send.at[d], recv_sem=flow_recv.at[d, c], **at(me + plane),
        )

    def sink(d, c):
        return pltpu.make_async_remote_copy(
            src_ref=qb.at[d, c], dst_ref=qb.at[d + 1, c],
            send_sem=flow_send.at[d], recv_sem=flow_recv.at[d, c], **at(me - plane),
        )

    def lift(d, c):
        return [
            pltpu.make_async_remote_copy(
                src_ref=up.at[d, c], dst_ref=down.at[d - 1, c],
                send_sem=lift_send.at[d, n], recv_sem=lift_recv.at[d - 1, c, n], **at(me + plane),
            )
            for n, (up, down) in enumerate(((up_o, down_o), (up_s, down_s)))
        ]

    def side(d, c, m):
        return pltpu.make_async_remote_copy(
            src_ref=stage.at[d, c, (m - 1) * CAP:m * CAP], dst_ref=picked.at[d, c, m * CAP:(m + 1) * CAP],
            send_sem=side_send.at[d], recv_sem=side_recv.at[d, c], **at(peer(m)),
        )

    def sides(d, c):
        return pltpu.make_async_remote_copy(
            src_ref=stage.at[d, c], dst_ref=picked.at[d, c, CAP:plane * CAP],
            send_sem=side_send.at[d], recv_sem=side_recv.at[d, c], **at(peer(1)),
        )

    def gather(m, c):
        return pltpu.make_async_remote_copy(
            src_ref=held.at[0, c], dst_ref=held.at[m, c],
            send_sem=side_send.at[m], recv_sem=side_recv.at[m, c], **at(peer(m)),
        )

    def project(i):
        mine = is_kv(i)
        c = i % heads

        pltpu.make_async_copy(w_all.at[i], w_all.at[i], w_sem.at[i % ahead]).wait()

        @pl.when(i + ahead < 2 * heads)
        def _():
            fetch(i + ahead)

        total = None
        for s in range(shares):
            owner = (core + s) % shares
            term = jnp.dot(
                parts[s], w_all[i, pl.ds(pl.multiple_of(owner * depth, depth), depth), :],
                preferred_element_type=jnp.float32,
            )
            total = term if total is None else total + term
        total = total.astype(jnp.bfloat16)

        @pl.when(mine)
        def _():
            held[0, c] = total.reshape(own_blocks, BLK, 2 * HD)

        @pl.when(jnp.logical_not(mine))
        def _():
            for g in range(group):
                qb[0, c, g * tok_rows:(g + 1) * tok_rows] = total[:, g * HD:(g + 1) * HD]

    def launch(c):
        @pl.when(climbs & above)
        def _():
            climb(0, c).start()

        if layers >= plane:
            @pl.when(spread)
            def _():
                for m in range(1, plane):
                    gather(m, c).start()

        @pl.when(sinks & below & ((top == 0) | (c < sent)))
        def _():
            sink(0, c).start()

    for copy in token_copies:
        copy.wait()
    project(0)

    pl.semaphore_wait(barrier, shares + plane - 2 + above.astype(jnp.int32) + jnp.where(sinks, layer * plane, 0))
    each_tell(lambda d: d <= layer, tell_all, lambda d: tell_bias(d).start())
    launch(0)

    def first_half(i, _):
        project(i)
        launch(i)
        return 0

    lax.fori_loop(1, heads, first_half, 0)

    def second_half(i, _):
        project(i)
        return 0

    lax.fori_loop(heads, 2 * heads, second_half, 0)
    fetch_out = pltpu.make_async_copy(wo_any, wo, wo_sem)
    fetch_out.start()
    acc[...] = jnp.zeros_like(acc)

    def attend(c, where_q, keys, values, mask):
        spans = [slice(g * tok_rows, (g + 1) * tok_rows) for g in range(group)]
        raw = [lax.dot_general(keys, qb[where_q, c, span], NT, preferred_element_type=jnp.float32) for span in spans]
        rounded = []
        for span, s in zip(spans, raw):
            s = mask(s.reshape(-1, BLK, tok_rows))
            peak = jnp.max(jnp.max(s, axis=0), axis=0, keepdims=True)
            p = jnp.exp2((s - peak[None]) * SCALE)
            fr_s[0:1, span] = peak
            fr_s[1:2, span] = jnp.sum(jnp.sum(p, axis=0), axis=0, keepdims=True)
            rounded.append(p.astype(jnp.bfloat16).reshape(-1, tok_rows))
        for span, p in zip(spans, rounded):
            fr_o[:, span] = lax.dot_general(values, p, TN, preferred_element_type=jnp.float32)

    def merge(o_a, s_a, o_b, s_b):
        peak = jnp.maximum(s_a[0:1], s_b[0:1])
        fac_a = jnp.exp2((s_a[0:1] - peak) * SCALE)
        fac_b = jnp.exp2((s_b[0:1] - peak) * SCALE)
        total = s_a[1:2] * fac_a + s_b[1:2] * fac_b
        return o_a.astype(jnp.float32) * fac_a + o_b * fac_b, peak, total

    def put(o_ref, s_ref, value):
        o, peak, total = value
        o_ref[...] = o.astype(o_ref.dtype)
        s_ref[0:1] = peak
        s_ref[1:2] = total

    def local(c):
        key_at = lax.broadcasted_iota(jnp.int32, (own_blocks, BLK, tok_rows), 0) * BLK + lax.broadcasted_iota(
            jnp.int32, (own_blocks, BLK, tok_rows), 1
        )
        query_at = lax.broadcasted_iota(jnp.int32, (own_blocks, BLK, tok_rows), 2)
        own_bias = own_bias_ref[0:own_blocks]

        def mask(s):
            return jnp.where(key_at > query_at, LOW, s + own_bias[:, None, :])

        attend(
            c, 0, held[0, c, :, :, 0:HD].reshape(tok_rows, HD), held[0, c, :, :, HD:2 * HD].reshape(tok_rows, HD), mask
        )
        st_o[c] = fr_o[...]
        st_s[c] = fr_s[...]

    def choose(source, c, block):
        taken = held[source, c, 0]
        for other in range(1, own_blocks):
            taken = jnp.where(block == other, held[source, c, other], taken)
        return taken

    def distribute(d, c):
        source = jnp.where(climbs, d, 0)
        table = jnp.where(climbs, 0, d)
        for m in range(1, plane):
            for place in range(CAP):
                stage[d, c, (m - 1) * CAP + place] = choose(source, c, asked_s[table, m, 0, (d * plane + m) * CAP + place])
            side(d, c, m).start()
        for place in range(CAP):
            picked[d, c, place] = choose(source, c, asked_s[table, 0, 0, d * plane * CAP + place])

    def turn(n):
        i = n // heads
        c = n % heads
        k = n - heads * (top - 1)
        paired = (k >= 0) & below & (top > 1)
        d = top - i
        d = jnp.where(paired, jnp.where(k % 2 == 0, 1, 0), d)
        c = jnp.where(paired, k // 2, c)
        if early > 0:
            m = n - early
            k = m - heads * (top - 2)
            low = jnp.where(k % 2 == 0, 2, 0)
            low = jnp.where((m < 0) | (k >= 2 * heads), 1, jnp.where(k >= 0, low, top - m // heads))
            at_low = jnp.where(k >= 2 * heads, k - 2 * heads + early, jnp.where(k >= 0, k // 2, m % heads))
            d = jnp.where(bottom, low, d)
            c = jnp.where(bottom, jnp.where(m < 0, n, at_low), c)
        return d, c

    busy = sinks & (top > 0)

    def pass_on(d, c):
        sink(d - 1, c).wait_recv()
        sink(d, c).start()

    def ready(c, _):
        @pl.when((busy & (c < jnp.where(top == 1, 1, top + 1) * heads)) | (climbs & (top == 0) & (c < heads)))
        def _():
            d, at_head = turn(c)

            @pl.when(jnp.logical_not(spread))
            def _():
                distribute(jnp.where(climbs, 0, d), jnp.where(climbs, c, at_head))

        return 0

    def to_scalars(first, last):
        move = pltpu.make_async_copy(asked.at[first:last], asked_s.at[first:last], move_sem)
        move.start()
        move.wait()

    tells(0).wait_recv()
    to_scalars(0, 1)

    @pl.when(sinks)
    def _():
        for d in range(1, layers):
            @pl.when(d <= top)
            def _():
                tells(d).wait_recv()
                tell_bias(d).wait_recv()

        if layers > 1:
            to_scalars(1, layers)

    lax.fori_loop(0, layers * heads, ready, 0)

    def forward(i, c):
        @pl.when(climbs & (i >= 1) & (i <= layer))
        def _():
            climb(i - 1, c).wait_recv()

            @pl.when(above)
            def _():
                climb(i, c).start()

        d = top - i

        @pl.when(sinks & below & (d >= 1))
        def _():
            pass_on(d, c)

        @pl.when(sinks & below & (d == 0) & (c == 0) & (top > 0))
        def _():
            def send(n, _):
                sink(0, n).start()
                return 0

            lax.fori_loop(sent, heads, send, 0)

    def finish(c):
        @pl.when(sinks & below)
        def _():
            for copy in lift(1, c):
                copy.wait_recv()
            put(st_o.at[c], st_s.at[c], merge(down_o[0, c], down_s[0, c], st_o[c], st_s[c]))

        for g in range(group):
            span = slice(g * tok_rows, (g + 1) * tok_rows)
            o = st_o[c, :, span] / st_s[c, 1:2, span]
            ho[0, c, :, g * HD:(g + 1) * HD] = o.T.astype(jnp.bfloat16)

        for share in range(1, shares):
            give(share, c).start()

    def give(share, c):
        return pltpu.make_async_remote_copy(
            src_ref=ho.at[0, c], dst_ref=ho.at[share, c],
            send_sem=give_send.at[share], recv_sem=give_recv.at[share, c], **at(me, (core + shares - share) % shares),
        )

    wide = group * HD
    out_cols = out_vmem.shape[1]
    tile = min(256, out_cols)

    def mixed_in(share, c, first):
        owner = (core + share) % shares
        rows_of = pl.multiple_of((owner * heads + c) * wide, wide)
        return jnp.dot(
            ho[share, c], wo[pl.ds(rows_of, wide), first:first + tile], preferred_element_type=jnp.float32
        )

    def add_in(c):
        for first in range(0, out_cols, tile):
            acc[:, first:first + tile] += mixed_in(0, c, first)

    def wait_blocks(d, c, fresh):
        if layers >= plane:
            @pl.when(spread)
            def _():
                @pl.when(fresh)
                def _():
                    for m in range(1, plane):
                        gather(m, c).wait_recv()

                for m in range(plane):
                    for place in range(CAP):
                        picked[d, c, m * CAP + place] = choose(m, c, asked_s[d, 0, 0, (d * plane + m) * CAP + place])

        @pl.when(jnp.logical_not(spread))
        def _():
            sides(d, c).wait_recv()

    def compute(d, c, fresh):
        away = sinks & (d >= 1)

        @pl.when(away & jnp.logical_not(below))
        def _():
            sink(d - 1, c).wait_recv()

        wait_blocks(d, c, fresh)
        group_bias = biasv[d]
        attend(
            c, jnp.where(climbs, 0, d),
            picked[d, c, :, :, 0:HD].reshape(cands * BLK, HD), picked[d, c, :, :, HD:2 * HD].reshape(cands * BLK, HD),
            lambda s: s + group_bias[:, None, :],
        )

        @pl.when(away)
        def _():
            @pl.when(below)
            def _():
                for copy in lift(d + 1, c):
                    copy.wait_recv()
                put(up_o.at[d, c], up_s.at[d, c], merge(down_o[d, c], down_s[d, c], fr_o[...], fr_s[...]))

            @pl.when(jnp.logical_not(below))
            def _():
                up_o[d, c] = fr_o[...].astype(jnp.bfloat16)
                up_s[d, c] = fr_s[...]

            for copy in lift(d, c):
                copy.start()

        @pl.when(jnp.logical_not(away))
        def _():
            put(st_o.at[c], st_s.at[c], merge(st_o[c], st_s[c], fr_o[...], fr_s[...]))

            @pl.when(climbs & (d == layer))
            def _():
                finish(c)
                add_in(c)

    hold = jnp.where(climbs, jnp.where(top >= 2, 2, jnp.where(above, 1, 0)), jnp.where((top == 0) & below, 1, 0))
    lag = jnp.where(bottom, 0, hold + jnp.where(climbs & (top == 1), 2, 1)) * heads
    fetch_out.wait()

    def step(n, _):
        i = n // heads
        c = n % heads

        @pl.when(i < layers)
        def _():
            forward(i, c)

        due = i - hold

        waits = gated & (climbs ^ (top == 0))

        @pl.when(waits & (n == hold * heads))
        def _():
            pl.semaphore_wait(go_sem, 1)

        @pl.when(gated & jnp.logical_not(waits) & (n == jnp.where(climbs, 3 * heads - heads // 2, jnp.where(below, 1, heads + heads // 4))))
        def _():
            pl.semaphore_signal(go_sem, inc=1, **at(me, mate))

        first_due = jnp.where(above, 0, 1)

        @pl.when((climbs & (due >= first_due) & (due <= layer)) | (sinks & (top == 0) & (due == 0)))
        def _():
            distribute(due, c)

        @pl.when(sinks & (top == 1) & (n == heads))
        def _():
            def each(h, _):
                distribute(0, h)
                return 0

            lax.fori_loop(0, heads, each, 0)

        @pl.when((i == 0) & jnp.logical_not(bottom))
        def _():
            local(c)

        @pl.when(bottom & (n == early))
        def _():
            def each(h, _):
                local(h)
                return 0

            lax.fori_loop(0, heads, each, 0)

        late = n - lag

        @pl.when((late >= 0) & (late < jnp.where(climbs, layer + 1, top + 1) * heads))
        def _():
            d, at_head = turn(late)
            fresh = (late < early) | ((late >= 2 * early) & (late < early + heads))
            compute(jnp.where(climbs, late // heads, d), jnp.where(climbs, late % heads, at_head), fresh)

        return 0

    lax.fori_loop(0, (layers + 3) * heads, step, 0)

    @pl.when(sinks)
    def _():
        def last(c, _):
            finish(c)
            add_in(c)
            return 0

        lax.fori_loop(0, heads, last, 0)

    def other(n, _):
        share = 1 + n // heads
        c = n % heads
        give(share, c).wait_recv()
        for first in range(0, out_cols, tile):
            acc[:, first:first + tile] += mixed_in(share, c, first)
        return 0

    total = (shares - 1) * heads
    lax.fori_loop(0, total - 1, other, 0)
    for share in range(max(shares - 1, 1), shares):
        give(share, heads - 1).wait_recv()
    for first in range(0, out_cols, tile):
        value = acc[:, first:first + tile]
        for share in range(max(shares - 1, 1), shares):
            value = value + mixed_in(share, heads - 1, first)
        out_vmem[:, first:first + tile] = value.astype(jnp.bfloat16)

    each_tell(lambda d: d <= layer, lambda d: tells(d).wait_send(), lambda d: tell_bias(d).wait_send())

    def sent_all(ref, sem):
        return pltpu.make_async_remote_copy(src_ref=ref, dst_ref=ref, send_sem=sem, recv_sem=sem, **at(peer(1)))

    def drain(d, _):
        @pl.when((climbs & (d <= layer)) | (sinks & (d <= top)))
        def _():
            @pl.when(jnp.logical_not(spread))
            def _():
                sent_all(stage.at[d], side_send.at[d]).wait_send()

            @pl.when(spread & (d >= 1) & (d < plane))
            def _():
                sent_all(held.at[0], side_send.at[d]).wait_send()

            @pl.when(climbs & above)
            def _():
                sent_all(held.at[d], flow_send.at[d]).wait_send()

            @pl.when(sinks & below)
            def _():
                sent_all(qb.at[d], flow_send.at[d]).wait_send()

            @pl.when(sinks & (d >= 1))
            def _():
                sent_all(up_o.at[d], lift_send.at[d, 0]).wait_send()
                sent_all(up_s.at[d], lift_send.at[d, 1]).wait_send()

        return 0

    lax.fori_loop(0, layers, drain, 0)
    for share in range(1, shares):
        sent_all(ho.at[0], give_send.at[share]).wait_send()


def attention(asks, bias, own_bias, parts, query_weight, key_weight, value_weight, out_weight, plane, layers):
    tok_rows, depth = parts[0].shape
    width, query_cols = query_weight.shape
    cols = key_weight.shape[1]
    heads = cols // HD
    group = query_cols // cols
    rows = group * tok_rows
    own_blocks = tok_rows // BLK
    out_cols = out_weight.shape[1]
    shares = len(parts)
    peers = plane - 1
    lanes = asks.shape[1]
    kind = parts[0].dtype
    dma = pltpu.SemaphoreType.DMA
    return pl.pallas_call(
        functools.partial(attention_kernel, plane, layers, shares),
        out_shape=jax.ShapeDtypeStruct((tok_rows, out_cols), kind),
        in_specs=[pl.BlockSpec(memory_space=VMEM)] * 3 + [pl.BlockSpec(memory_space=pl.ANY)] * (4 + shares),
        out_specs=pl.BlockSpec(memory_space=VMEM),
        scratch_shapes=[
            pltpu.VMEM((layers, heads, own_blocks, BLK, 2 * HD), kind),
            pltpu.VMEM((layers, heads, rows, HD), kind),
            pltpu.VMEM((layers, heads, plane * CAP, BLK, 2 * HD), kind),
            pltpu.VMEM((layers, heads, peers * CAP, BLK, 2 * HD), kind),
            pltpu.VMEM((layers, heads, HD, rows), kind),
            pltpu.VMEM((layers, heads, 2, rows), jnp.float32),
            pltpu.VMEM((layers, heads, HD, rows), kind),
            pltpu.VMEM((layers, heads, 2, rows), jnp.float32),
            pltpu.VMEM((heads, HD, rows), jnp.float32),
            pltpu.VMEM((heads, 2, rows), jnp.float32),
            pltpu.VMEM((HD, rows), jnp.float32),
            pltpu.VMEM((2, rows), jnp.float32),
            pltpu.VMEM((layers, plane, 1, lanes), jnp.int32),
            pltpu.SMEM((layers, plane, 1, lanes), jnp.int32),
            pltpu.VMEM(bias.shape, jnp.float32),
            pltpu.VMEM((2 * heads, width, group * HD), kind),
            pltpu.VMEM((shares, tok_rows, depth), kind),
            pltpu.VMEM(out_weight.shape, kind),
            pltpu.VMEM((shares, heads, tok_rows, group * HD), kind),
            pltpu.VMEM((tok_rows, out_cols), jnp.float32),
            dma((min(3, 2 * heads),)), dma((shares,)), pltpu.SemaphoreType.REGULAR,
            dma((layers,)), dma((layers,)), dma((layers,)), dma((layers,)), dma(()),
            dma((layers,)), dma((layers, heads)), dma((layers,)), dma((layers, heads)),
            dma((layers, 2)), dma((layers, heads, 2)),
            dma(()), dma((shares,)), dma((shares, heads)),
        ],
        compiler_params=pltpu.CompilerParams(
            collective_id=0, has_side_effects=True, vmem_limit_bytes=53 * 2**20
        ),
    )(asks, bias, own_bias, query_weight, key_weight, value_weight, out_weight, *parts)


def turned(x, shift):
    size = lax.axis_size("tp")
    return lax.ppermute(x, "tp", [((i + shift) % size, i) for i in range(size)])


def shares_of(x):
    size = lax.axis_size("tp")
    me = lax.axis_index("tp")
    return [(x if s == 0 else turned(x, s), (me + s) % size) for s in range(size)]


def tables(chosen, plane, layers):
    own_blocks = chosen.shape[0]
    device = lax.axis_index("kv")
    layer = lax.div(device, jnp.int32(plane))
    seat = device - layer * plane
    holder = lax.div(chosen, jnp.int32(own_blocks))
    within = chosen - holder * own_blocks
    holder_layer = lax.div(holder, jnp.int32(plane))
    owner = (layer - holder_layer) * plane + ((holder - holder_layer * plane) ^ seat)
    count = layers * plane
    ids = jnp.arange(count, dtype=jnp.int32)
    hit = owner.reshape(1, -1) == ids[:, None]
    low = jnp.min(jnp.where(hit, within.reshape(1, -1), own_blocks), axis=1)
    high = jnp.max(jnp.where(hit, within.reshape(1, -1), -1), axis=1)
    asks = jnp.stack([jnp.where(low < own_blocks, low, 0), jnp.maximum(high, 0)], axis=1).reshape(1, -1)
    lanes = -(-asks.shape[1] // 128) * 128
    asks = jnp.pad(asks, ((0, 0), (0, lanes - asks.shape[1])))
    far = ids >= 1
    names = jnp.stack(
        [
            jnp.where(far & (low < own_blocks), ids * own_blocks + low, -1),
            jnp.where(far & (high > low), ids * own_blocks + high, -1),
        ],
        axis=1,
    ).reshape(-1)
    names = jnp.concatenate([names, jnp.arange(8, dtype=jnp.int32)])
    wanted = jnp.repeat(jnp.transpose(owner * own_blocks + within), BLK, axis=1)
    seen = jnp.any(wanted[None] == names[:, None, None], axis=1)
    bias = jnp.where(seen, 0.0, LOW).astype(jnp.float32)
    cut = count * CAP
    return asks, bias[:cut].reshape(layers, plane * CAP, -1), bias[cut:]


def local(tokens, query_weight, key_weight, value_weight, out_weight, chosen):
    key_devices = lax.axis_size("kv")
    plane = math.gcd(key_devices, PLANE)
    layers = key_devices // plane
    asks, bias, own_bias = tables(chosen, plane, layers)
    parts = [block for block, _ in shares_of(tokens)]
    return attention(
        asks, bias, own_bias, parts, query_weight, key_weight, value_weight, out_weight, plane, layers
    )


def solution(mesh):
    return jax.shard_map(
        local,
        mesh=mesh,
        in_specs=(
            P("kv", "tp"),
            P(None, "tp"),
            P(None, "tp"),
            P(None, "tp"),
            P(None, "tp"),
            P("kv", None),
        ),
        out_specs=P("kv", "tp"),
        check_vma=False,
    )
```

```python
import functools
import math

import jax
import jax.numpy as jnp
from jax import lax
from jax.experimental import pallas as pl
from jax.experimental.pallas import tpu as pltpu
from jax.sharding import PartitionSpec as P

HD = 128
BLK = 64
CAP = 2
PLANE = 4
LOW = -1e30
SCALE = HD ** (-0.5) * math.log2(math.e)
VMEM = pltpu.MemorySpace.VMEM
SMEM = pltpu.MemorySpace.SMEM
NT = (((1,), (1,)), ((), ()))
TN = (((0,), (0,)), ((), ()))


def attention_kernel(
    plane, layers, shares,
    asks_ref, bias_ref, own_bias_ref, wq_any, wk_any, wv_any, wo_any, *refs,
):
    parts = refs[:shares]
    (
        out_vmem,
        held, qb, picked, stage, up_o, up_s, down_o, down_s, st_o, st_s, fr_o, fr_s,
        asked, asked_s, biasv, w_all, wo, ho, acc,
        w_sem, go_sem, tell_send, tell_recv, bias_send, bias_recv, move_sem,
        flow_send, flow_recv, side_send, side_recv, lift_send, lift_recv, wo_sem, give_send, give_recv,
    ) = refs[shares:]
    heads, own_blocks = held.shape[1], held.shape[2]
    tok_rows = own_blocks * BLK
    rows = qb.shape[2]
    group = rows // tok_rows
    depth = parts[0].shape[1]
    cands = plane * CAP
    me = lax.axis_index("kv")
    core = lax.axis_index("tp")
    layer = me // plane
    seat = me % plane
    climbs = core % 2 == 0
    sinks = core % 2 == 1
    above = layer + 1 < layers
    below = layer > 0
    top = layers - 1 - layer
    early = min(2, heads) if layers > 2 else 0
    sent = jnp.where(layer == 1, early, 0)
    bottom = sinks & jnp.logical_not(below) & (top > 0)
    spread = bottom & (layers >= plane)

    def at(device, lane=None):
        return {
            "device_id": {"kv": device, "tp": core if lane is None else lane},
            "device_id_type": pl.DeviceIdType.MESH,
        }

    def peer(m):
        return layer * plane + (seat ^ m)

    ahead = min(3, 2 * heads)

    def weight_copies(i):
        c = i % heads
        wide = group * HD
        kv = [
            pltpu.make_async_copy(
                wk_any.at[:, pl.ds(pl.multiple_of(c * HD, HD), HD)], w_all.at[i, :, 0:HD], w_sem.at[i % ahead]
            ),
            pltpu.make_async_copy(
                wv_any.at[:, pl.ds(pl.multiple_of(c * HD, HD), HD)], w_all.at[i, :, HD:2 * HD], w_sem.at[i % ahead]
            ),
        ]
        q = [
            pltpu.make_async_copy(
                wq_any.at[:, pl.ds(pl.multiple_of(c * wide, HD), wide)], w_all.at[i], w_sem.at[i % ahead]
            )
        ]
        return kv, q

    def is_kv(i):
        keys_first = climbs | spread
        return ((i < heads) & keys_first) | ((i >= heads) & jnp.logical_not(keys_first))

    def fetch(i):
        kv, q = weight_copies(i)

        @pl.when(is_kv(i))
        def _():
            for copy in kv:
                copy.start()

        @pl.when(jnp.logical_not(is_kv(i)))
        def _():
            for copy in q:
                copy.start()

    for i in range(ahead):
        fetch(i)

    asked[...] = jnp.zeros_like(asked)
    asked[0, 0] = asks_ref[...]
    biasv[0] = bias_ref[0]

    @pl.when(climbs)
    def _():
        for d in range(1, layers):
            biasv[d] = bias_ref[d]

    barrier = pltpu.get_barrier_semaphore()
    gated = ((top >= 2) | (top == 0)) & (core + jnp.where(climbs, 1, 0) < shares)
    mate = core + 1 - 2 * (core % 2)
    for share in range(1, shares):
        pl.semaphore_signal(barrier, inc=1, **at(me, (core + share) % shares))

    for m in range(1, plane):
        pl.semaphore_signal(barrier, inc=1, **at(peer(m)))

    @pl.when(below)
    def _():
        pl.semaphore_signal(barrier, inc=1, **at(me - plane))

    @pl.when(sinks)
    def _():
        def greet(device, _):
            pl.semaphore_signal(barrier, inc=1, **at(device))
            return 0

        lax.fori_loop((layer + 1) * plane, layers * plane, greet, 0)

    def tell(d, m):
        return pltpu.make_async_remote_copy(
            src_ref=asks_ref, dst_ref=asked.at[d, m], send_sem=tell_send.at[d], recv_sem=tell_recv.at[d],
            **at((layer - d) * plane + (seat ^ m)),
        )

    def tell_bias(d):
        return pltpu.make_async_remote_copy(
            src_ref=bias_ref.at[d], dst_ref=biasv.at[d], send_sem=bias_send.at[d], recv_sem=bias_recv.at[d],
            **at(me - d * plane),
        )

    def tells(d):
        first = 1 if d == 0 else 0
        span = asked.at[d, first:plane]
        return pltpu.make_async_remote_copy(
            src_ref=span, dst_ref=span, send_sem=tell_send.at[d], recv_sem=tell_recv.at[d], **at(me - d * plane)
            if d else at(peer(1)),
        )

    def each_tell(far, act, bias_act):
        act(0)
        for d in range(1, layers):
            @pl.when(sinks & far(d))
            def _():
                act(d)
                bias_act(d)

    def tell_all(d):
        for m in range(1 if d == 0 else 0, plane):
            tell(d, m).start()

    def climb(d, c):
        return pltpu.make_async_remote_copy(
            src_ref=held.at[d, c], dst_ref=held.at[d + 1, c],
            send_sem=flow_send.at[d], recv_sem=flow_recv.at[d, c], **at(me + plane),
        )

    def sink(d, c):
        return pltpu.make_async_remote_copy(
            src_ref=qb.at[d, c], dst_ref=qb.at[d + 1, c],
            send_sem=flow_send.at[d], recv_sem=flow_recv.at[d, c], **at(me - plane),
        )

    def lift(d, c):
        return [
            pltpu.make_async_remote_copy(
                src_ref=up.at[d, c], dst_ref=down.at[d - 1, c],
                send_sem=lift_send.at[d, n], recv_sem=lift_recv.at[d - 1, c, n], **at(me + plane),
            )
            for n, (up, down) in enumerate(((up_o, down_o), (up_s, down_s)))
        ]

    def side(d, c, m):
        return pltpu.make_async_remote_copy(
            src_ref=stage.at[d, c, (m - 1) * CAP:m * CAP], dst_ref=picked.at[d, c, m * CAP:(m + 1) * CAP],
            send_sem=side_send.at[d], recv_sem=side_recv.at[d, c], **at(peer(m)),
        )

    def sides(d, c):
        return pltpu.make_async_remote_copy(
            src_ref=stage.at[d, c], dst_ref=picked.at[d, c, CAP:plane * CAP],
            send_sem=side_send.at[d], recv_sem=side_recv.at[d, c], **at(peer(1)),
        )

    def gather(m, c):
        return pltpu.make_async_remote_copy(
            src_ref=held.at[0, c], dst_ref=held.at[m, c],
            send_sem=side_send.at[m], recv_sem=side_recv.at[m, c], **at(peer(m)),
        )

    def project(i):
        mine = is_kv(i)
        c = i % heads

        pltpu.make_async_copy(w_all.at[i], w_all.at[i], w_sem.at[i % ahead]).wait()

        @pl.when(i + ahead < 2 * heads)
        def _():
            fetch(i + ahead)

        total = None
        for s in range(shares):
            owner = (core + s) % shares
            term = jnp.dot(
                parts[s][...], w_all[i, pl.ds(pl.multiple_of(owner * depth, depth), depth), :],
                preferred_element_type=jnp.float32,
            )
            total = term if total is None else total + term
        total = total.astype(jnp.bfloat16)

        @pl.when(mine)
        def _():
            held[0, c] = total.reshape(own_blocks, BLK, 2 * HD)

        @pl.when(jnp.logical_not(mine))
        def _():
            for g in range(group):
                qb[0, c, g * tok_rows:(g + 1) * tok_rows] = total[:, g * HD:(g + 1) * HD]

    def launch(c):
        @pl.when(climbs & above)
        def _():
            climb(0, c).start()

        if layers >= plane:
            @pl.when(spread)
            def _():
                for m in range(1, plane):
                    gather(m, c).start()

        @pl.when(sinks & below & ((top == 0) | (c < sent)))
        def _():
            sink(0, c).start()

    project(0)

    pl.semaphore_wait(barrier, shares + plane - 2 + above.astype(jnp.int32) + jnp.where(sinks, layer * plane, 0))
    each_tell(lambda d: d <= layer, tell_all, lambda d: tell_bias(d).start())
    launch(0)

    def first_half(i, _):
        project(i)
        launch(i)
        return 0

    lax.fori_loop(1, heads, first_half, 0)

    def second_half(i, _):
        project(i)
        return 0

    lax.fori_loop(heads, 2 * heads, second_half, 0)
    fetch_out = pltpu.make_async_copy(wo_any, wo, wo_sem)
    fetch_out.start()
    acc[...] = jnp.zeros_like(acc)

    def attend(c, where_q, keys, values, mask):
        spans = [slice(g * tok_rows, (g + 1) * tok_rows) for g in range(group)]
        raw = [lax.dot_general(keys, qb[where_q, c, span], NT, preferred_element_type=jnp.float32) for span in spans]
        rounded = []
        for span, s in zip(spans, raw):
            s = mask(s.reshape(-1, BLK, tok_rows))
            peak = jnp.max(jnp.max(s, axis=0), axis=0, keepdims=True)
            p = jnp.exp2((s - peak[None]) * SCALE)
            fr_s[0:1, span] = peak
            fr_s[1:2, span] = jnp.sum(jnp.sum(p, axis=0), axis=0, keepdims=True)
            rounded.append(p.astype(jnp.bfloat16).reshape(-1, tok_rows))
        for span, p in zip(spans, rounded):
            fr_o[:, span] = lax.dot_general(values, p, TN, preferred_element_type=jnp.float32)

    def merge(o_a, s_a, o_b, s_b):
        peak = jnp.maximum(s_a[0:1], s_b[0:1])
        fac_a = jnp.exp2((s_a[0:1] - peak) * SCALE)
        fac_b = jnp.exp2((s_b[0:1] - peak) * SCALE)
        total = s_a[1:2] * fac_a + s_b[1:2] * fac_b
        return o_a.astype(jnp.float32) * fac_a + o_b * fac_b, peak, total

    def put(o_ref, s_ref, value):
        o, peak, total = value
        o_ref[...] = o.astype(o_ref.dtype)
        s_ref[0:1] = peak
        s_ref[1:2] = total

    def local(c):
        key_at = lax.broadcasted_iota(jnp.int32, (own_blocks, BLK, tok_rows), 0) * BLK + lax.broadcasted_iota(
            jnp.int32, (own_blocks, BLK, tok_rows), 1
        )
        query_at = lax.broadcasted_iota(jnp.int32, (own_blocks, BLK, tok_rows), 2)
        own_bias = own_bias_ref[0:own_blocks]

        def mask(s):
            return jnp.where(key_at > query_at, LOW, s + own_bias[:, None, :])

        attend(
            c, 0, held[0, c, :, :, 0:HD].reshape(tok_rows, HD), held[0, c, :, :, HD:2 * HD].reshape(tok_rows, HD), mask
        )
        st_o[c] = fr_o[...]
        st_s[c] = fr_s[...]

    def choose(source, c, block):
        taken = held[source, c, 0]
        for other in range(1, own_blocks):
            taken = jnp.where(block == other, held[source, c, other], taken)
        return taken

    def distribute(d, c):
        source = jnp.where(climbs, d, 0)
        table = jnp.where(climbs, 0, d)
        for m in range(1, plane):
            for place in range(CAP):
                stage[d, c, (m - 1) * CAP + place] = choose(source, c, asked_s[table, m, 0, (d * plane + m) * CAP + place])
            side(d, c, m).start()
        for place in range(CAP):
            picked[d, c, place] = choose(source, c, asked_s[table, 0, 0, d * plane * CAP + place])

    def turn(n):
        i = n // heads
        c = n % heads
        k = n - heads * (top - 1)
        paired = (k >= 0) & below & (top > 1)
        d = top - i
        d = jnp.where(paired, jnp.where(k % 2 == 0, 1, 0), d)
        c = jnp.where(paired, k // 2, c)
        if early > 0:
            m = n - early
            k = m - heads * (top - 2)
            low = jnp.where(k % 2 == 0, 2, 0)
            low = jnp.where((m < 0) | (k >= 2 * heads), 1, jnp.where(k >= 0, low, top - m // heads))
            at_low = jnp.where(k >= 2 * heads, k - 2 * heads + early, jnp.where(k >= 0, k // 2, m % heads))
            d = jnp.where(bottom, low, d)
            c = jnp.where(bottom, jnp.where(m < 0, n, at_low), c)
        return d, c

    busy = sinks & (top > 0)

    def pass_on(d, c):
        sink(d - 1, c).wait_recv()
        sink(d, c).start()

    def ready(c, _):
        @pl.when((busy & (c < jnp.where(top == 1, 1, top + 1) * heads)) | (climbs & (top == 0) & (c < heads)))
        def _():
            d, at_head = turn(c)

            @pl.when(jnp.logical_not(spread))
            def _():
                distribute(jnp.where(climbs, 0, d), jnp.where(climbs, c, at_head))

        return 0

    def to_scalars(first, last):
        move = pltpu.make_async_copy(asked.at[first:last], asked_s.at[first:last], move_sem)
        move.start()
        move.wait()

    tells(0).wait_recv()
    to_scalars(0, 1)

    @pl.when(sinks)
    def _():
        for d in range(1, layers):
            @pl.when(d <= top)
            def _():
                tells(d).wait_recv()
                tell_bias(d).wait_recv()

        if layers > 1:
            to_scalars(1, layers)

    lax.fori_loop(0, layers * heads, ready, 0)

    def forward(i, c):
        @pl.when(climbs & (i >= 1) & (i <= layer))
        def _():
            climb(i - 1, c).wait_recv()

            @pl.when(above)
            def _():
                climb(i, c).start()

        d = top - i

        @pl.when(sinks & below & (d >= 1))
        def _():
            pass_on(d, c)

        @pl.when(sinks & below & (d == 0) & (c == 0) & (top > 0))
        def _():
            def send(n, _):
                sink(0, n).start()
                return 0

            lax.fori_loop(sent, heads, send, 0)

    def finish(c):
        @pl.when(sinks & below)
        def _():
            for copy in lift(1, c):
                copy.wait_recv()
            put(st_o.at[c], st_s.at[c], merge(down_o[0, c], down_s[0, c], st_o[c], st_s[c]))

        for g in range(group):
            span = slice(g * tok_rows, (g + 1) * tok_rows)
            o = st_o[c, :, span] / st_s[c, 1:2, span]
            ho[0, c, :, g * HD:(g + 1) * HD] = o.T.astype(jnp.bfloat16)

        for share in range(1, shares):
            give(share, c).start()

    def give(share, c):
        return pltpu.make_async_remote_copy(
            src_ref=ho.at[0, c], dst_ref=ho.at[share, c],
            send_sem=give_send.at[share], recv_sem=give_recv.at[share, c], **at(me, (core + shares - share) % shares),
        )

    wide = group * HD
    out_cols = out_vmem.shape[1]
    tile = min(256, out_cols)

    def mixed_in(share, c, first):
        owner = (core + share) % shares
        rows_of = pl.multiple_of((owner * heads + c) * wide, wide)
        return jnp.dot(
            ho[share, c], wo[pl.ds(rows_of, wide), first:first + tile], preferred_element_type=jnp.float32
        )

    def add_in(c):
        for first in range(0, out_cols, tile):
            acc[:, first:first + tile] += mixed_in(0, c, first)

    def wait_blocks(d, c, fresh):
        if layers >= plane:
            @pl.when(spread)
            def _():
                @pl.when(fresh)
                def _():
                    for m in range(1, plane):
                        gather(m, c).wait_recv()

                for m in range(plane):
                    for place in range(CAP):
                        picked[d, c, m * CAP + place] = choose(m, c, asked_s[d, 0, 0, (d * plane + m) * CAP + place])

        @pl.when(jnp.logical_not(spread))
        def _():
            sides(d, c).wait_recv()

    def compute(d, c, fresh):
        away = sinks & (d >= 1)

        @pl.when(away & jnp.logical_not(below))
        def _():
            sink(d - 1, c).wait_recv()

        wait_blocks(d, c, fresh)
        group_bias = biasv[d]
        attend(
            c, jnp.where(climbs, 0, d),
            picked[d, c, :, :, 0:HD].reshape(cands * BLK, HD), picked[d, c, :, :, HD:2 * HD].reshape(cands * BLK, HD),
            lambda s: s + group_bias[:, None, :],
        )

        @pl.when(away)
        def _():
            @pl.when(below)
            def _():
                for copy in lift(d + 1, c):
                    copy.wait_recv()
                put(up_o.at[d, c], up_s.at[d, c], merge(down_o[d, c], down_s[d, c], fr_o[...], fr_s[...]))

            @pl.when(jnp.logical_not(below))
            def _():
                up_o[d, c] = fr_o[...].astype(jnp.bfloat16)
                up_s[d, c] = fr_s[...]

            for copy in lift(d, c):
                copy.start()

        @pl.when(jnp.logical_not(away))
        def _():
            put(st_o.at[c], st_s.at[c], merge(st_o[c], st_s[c], fr_o[...], fr_s[...]))

            @pl.when(climbs & (d == layer))
            def _():
                finish(c)
                add_in(c)

    hold = jnp.where(climbs, jnp.where(top >= 2, 2, jnp.where(above, 1, 0)), jnp.where((top == 0) & below, 1, 0))
    lag = jnp.where(bottom, 0, hold + jnp.where(climbs & (top == 1), 2, 1)) * heads
    fetch_out.wait()

    def step(n, _):
        i = n // heads
        c = n % heads

        @pl.when(i < layers)
        def _():
            forward(i, c)

        due = i - hold

        waits = gated & (climbs ^ (top == 0))

        @pl.when(waits & (n == hold * heads))
        def _():
            pl.semaphore_wait(go_sem, 1)

        @pl.when(gated & jnp.logical_not(waits) & (n == jnp.where(climbs, 3 * heads - heads // 2, jnp.where(below, 1, heads + heads // 4))))
        def _():
            pl.semaphore_signal(go_sem, inc=1, **at(me, mate))

        first_due = jnp.where(above, 0, 1)

        @pl.when((climbs & (due >= first_due) & (due <= layer)) | (sinks & (top == 0) & (due == 0)))
        def _():
            distribute(due, c)

        @pl.when(sinks & (top == 1) & (n == heads))
        def _():
            def each(h, _):
                distribute(0, h)
                return 0

            lax.fori_loop(0, heads, each, 0)

        @pl.when((i == 0) & jnp.logical_not(bottom))
        def _():
            local(c)

        @pl.when(bottom & (n == early))
        def _():
            def each(h, _):
                local(h)
                return 0

            lax.fori_loop(0, heads, each, 0)

        late = n - lag

        @pl.when((late >= 0) & (late < jnp.where(climbs, layer + 1, top + 1) * heads))
        def _():
            d, at_head = turn(late)
            fresh = (late < early) | ((late >= 2 * early) & (late < early + heads))
            compute(jnp.where(climbs, late // heads, d), jnp.where(climbs, late % heads, at_head), fresh)

        return 0

    lax.fori_loop(0, (layers + 3) * heads, step, 0)

    @pl.when(sinks)
    def _():
        def last(c, _):
            finish(c)
            add_in(c)
            return 0

        lax.fori_loop(0, heads, last, 0)

    def other(n, _):
        share = 1 + n // heads
        c = n % heads
        give(share, c).wait_recv()
        for first in range(0, out_cols, tile):
            acc[:, first:first + tile] += mixed_in(share, c, first)
        return 0

    total = (shares - 1) * heads
    lax.fori_loop(0, total - 1, other, 0)
    for share in range(max(shares - 1, 1), shares):
        give(share, heads - 1).wait_recv()
    for first in range(0, out_cols, tile):
        value = acc[:, first:first + tile]
        for share in range(max(shares - 1, 1), shares):
            value = value + mixed_in(share, heads - 1, first)
        out_vmem[:, first:first + tile] = value.astype(jnp.bfloat16)

    each_tell(lambda d: d <= layer, lambda d: tells(d).wait_send(), lambda d: tell_bias(d).wait_send())

    def sent_all(ref, sem):
        return pltpu.make_async_remote_copy(src_ref=ref, dst_ref=ref, send_sem=sem, recv_sem=sem, **at(peer(1)))

    def drain(d, _):
        @pl.when((climbs & (d <= layer)) | (sinks & (d <= top)))
        def _():
            @pl.when(jnp.logical_not(spread))
            def _():
                sent_all(stage.at[d], side_send.at[d]).wait_send()

            @pl.when(spread & (d >= 1) & (d < plane))
            def _():
                sent_all(held.at[0], side_send.at[d]).wait_send()

            @pl.when(climbs & above)
            def _():
                sent_all(held.at[d], flow_send.at[d]).wait_send()

            @pl.when(sinks & below)
            def _():
                sent_all(qb.at[d], flow_send.at[d]).wait_send()

            @pl.when(sinks & (d >= 1))
            def _():
                sent_all(up_o.at[d], lift_send.at[d, 0]).wait_send()
                sent_all(up_s.at[d], lift_send.at[d, 1]).wait_send()

        return 0

    lax.fori_loop(0, layers, drain, 0)
    for share in range(1, shares):
        sent_all(ho.at[0], give_send.at[share]).wait_send()


def attention(asks, bias, own_bias, parts, query_weight, key_weight, value_weight, out_weight, plane, layers):
    tok_rows, depth = parts[0].shape
    width, query_cols = query_weight.shape
    cols = key_weight.shape[1]
    heads = cols // HD
    group = query_cols // cols
    rows = group * tok_rows
    own_blocks = tok_rows // BLK
    out_cols = out_weight.shape[1]
    shares = len(parts)
    peers = plane - 1
    lanes = asks.shape[1]
    kind = parts[0].dtype
    dma = pltpu.SemaphoreType.DMA
    return pl.pallas_call(
        functools.partial(attention_kernel, plane, layers, shares),
        out_shape=jax.ShapeDtypeStruct((tok_rows, out_cols), kind),
        in_specs=[pl.BlockSpec(memory_space=VMEM)] * 3 + [pl.BlockSpec(memory_space=pl.ANY)] * 4
        + [pl.BlockSpec(memory_space=VMEM)] * shares,
        out_specs=pl.BlockSpec(memory_space=VMEM),
        scratch_shapes=[
            pltpu.VMEM((layers, heads, own_blocks, BLK, 2 * HD), kind),
            pltpu.VMEM((layers, heads, rows, HD), kind),
            pltpu.VMEM((layers, heads, plane * CAP, BLK, 2 * HD), kind),
            pltpu.VMEM((layers, heads, peers * CAP, BLK, 2 * HD), kind),
            pltpu.VMEM((layers, heads, HD, rows), kind),
            pltpu.VMEM((layers, heads, 2, rows), jnp.float32),
            pltpu.VMEM((layers, heads, HD, rows), kind),
            pltpu.VMEM((layers, heads, 2, rows), jnp.float32),
            pltpu.VMEM((heads, HD, rows), jnp.float32),
            pltpu.VMEM((heads, 2, rows), jnp.float32),
            pltpu.VMEM((HD, rows), jnp.float32),
            pltpu.VMEM((2, rows), jnp.float32),
            pltpu.VMEM((layers, plane, 1, lanes), jnp.int32),
            pltpu.SMEM((layers, plane, 1, lanes), jnp.int32),
            pltpu.VMEM(bias.shape, jnp.float32),
            pltpu.VMEM((2 * heads, width, group * HD), kind),
            pltpu.VMEM(out_weight.shape, kind),
            pltpu.VMEM((shares, heads, tok_rows, group * HD), kind),
            pltpu.VMEM((tok_rows, out_cols), jnp.float32),
            dma((min(3, 2 * heads),)), pltpu.SemaphoreType.REGULAR,
            dma((layers,)), dma((layers,)), dma((layers,)), dma((layers,)), dma(()),
            dma((layers,)), dma((layers, heads)), dma((layers,)), dma((layers, heads)),
            dma((layers, 2)), dma((layers, heads, 2)),
            dma(()), dma((shares,)), dma((shares, heads)),
        ],
        compiler_params=pltpu.CompilerParams(
            collective_id=0, has_side_effects=True, vmem_limit_bytes=51 * 2**20
        ),
    )(asks, bias, own_bias, query_weight, key_weight, value_weight, out_weight, *parts)


def turned(x, shift):
    size = lax.axis_size("tp")
    return lax.ppermute(x, "tp", [((i + shift) % size, i) for i in range(size)])


def shares_of(x):
    size = lax.axis_size("tp")
    me = lax.axis_index("tp")
    return [(x if s == 0 else turned(x, s), (me + s) % size) for s in range(size)]


def tables(chosen, plane, layers):
    own_blocks = chosen.shape[0]
    device = lax.axis_index("kv")
    layer = lax.div(device, jnp.int32(plane))
    seat = device - layer * plane
    holder = lax.div(chosen, jnp.int32(own_blocks))
    within = chosen - holder * own_blocks
    holder_layer = lax.div(holder, jnp.int32(plane))
    owner = (layer - holder_layer) * plane + ((holder - holder_layer * plane) ^ seat)
    count = layers * plane
    ids = jnp.arange(count, dtype=jnp.int32)
    hit = owner.reshape(1, -1) == ids[:, None]
    low = jnp.min(jnp.where(hit, within.reshape(1, -1), own_blocks), axis=1)
    high = jnp.max(jnp.where(hit, within.reshape(1, -1), -1), axis=1)
    asks = jnp.stack([jnp.where(low < own_blocks, low, 0), jnp.maximum(high, 0)], axis=1).reshape(1, -1)
    lanes = -(-asks.shape[1] // 128) * 128
    asks = jnp.pad(asks, ((0, 0), (0, lanes - asks.shape[1])))
    far = ids >= 1
    names = jnp.stack(
        [
            jnp.where(far & (low < own_blocks), ids * own_blocks + low, -1),
            jnp.where(far & (high > low), ids * own_blocks + high, -1),
        ],
        axis=1,
    ).reshape(-1)
    names = jnp.concatenate([names, jnp.arange(8, dtype=jnp.int32)])
    wanted = jnp.repeat(jnp.transpose(owner * own_blocks + within), BLK, axis=1)
    seen = jnp.any(wanted[None] == names[:, None, None], axis=1)
    bias = jnp.where(seen, 0.0, LOW).astype(jnp.float32)
    cut = count * CAP
    return asks, bias[:cut].reshape(layers, plane * CAP, -1), bias[cut:]


def local(tokens, query_weight, key_weight, value_weight, out_weight, chosen):
    key_devices = lax.axis_size("kv")
    plane = math.gcd(key_devices, PLANE)
    layers = key_devices // plane
    asks, bias, own_bias = tables(chosen, plane, layers)
    parts = [block for block, _ in shares_of(tokens)]
    return attention(
        asks, bias, own_bias, parts, query_weight, key_weight, value_weight, out_weight, plane, layers
    )


def solution(mesh):
    return jax.shard_map(
        local,
        mesh=mesh,
        in_specs=(
            P("kv", "tp"),
            P(None, "tp"),
            P(None, "tp"),
            P(None, "tp"),
            P(None, "tp"),
            P("kv", None),
        ),
        out_specs=P("kv", "tp"),
        check_vma=False,
    )
```

```python
import functools
import math

import jax
import jax.numpy as jnp
from jax import lax
from jax.experimental import pallas as pl
from jax.experimental.pallas import tpu as pltpu
from jax.sharding import PartitionSpec as P

HD = 128
BLK = 64
CAP = 2
PLANE = 4
LOW = -1e30
SCALE = HD ** (-0.5) * math.log2(math.e)
VMEM = pltpu.MemorySpace.VMEM
SMEM = pltpu.MemorySpace.SMEM
NT = (((1,), (1,)), ((), ()))
TN = (((0,), (0,)), ((), ()))


def attention_kernel(
    plane, layers, shares,
    asks_ref, bias_ref, own_bias_ref, wq_any, wk_any, wv_any, wo_any, *refs,
):
    parts = refs[:shares]
    (
        out_vmem,
        held, qb, picked, stage, up_o, up_s, down_o, down_s, st_o, st_s, fr_o, fr_s,
        asked, asked_s, biasv, w_all, wo, ho, acc,
        w_sem, go_sem, tell_send, tell_recv, bias_send, bias_recv, move_sem,
        flow_send, flow_recv, side_send, side_recv, lift_send, lift_recv, wo_sem, give_send, give_recv,
    ) = refs[shares:]
    heads, own_blocks = held.shape[1], held.shape[2]
    tok_rows = own_blocks * BLK
    rows = qb.shape[2]
    group = rows // tok_rows
    depth = parts[0].shape[1]
    cands = plane * CAP
    me = lax.axis_index("kv")
    core = lax.axis_index("tp")
    layer = me // plane
    seat = me % plane
    climbs = core % 2 == 0
    sinks = core % 2 == 1
    above = layer + 1 < layers
    below = layer > 0
    top = layers - 1 - layer
    early = min(2, heads) if layers > 2 else 0
    sent = jnp.where(layer == 1, early, 0)
    bottom = sinks & jnp.logical_not(below) & (top > 0)
    spread = bottom & (layers >= plane)

    def at(device, lane=None):
        return {
            "device_id": {"kv": device, "tp": core if lane is None else lane},
            "device_id_type": pl.DeviceIdType.MESH,
        }

    def peer(m):
        return layer * plane + (seat ^ m)

    ahead = min(3, 2 * heads)

    def weight_copies(i):
        c = i % heads
        wide = group * HD
        kv = [
            pltpu.make_async_copy(
                wk_any.at[:, pl.ds(pl.multiple_of(c * HD, HD), HD)], w_all.at[i, :, 0:HD], w_sem.at[i % ahead]
            ),
            pltpu.make_async_copy(
                wv_any.at[:, pl.ds(pl.multiple_of(c * HD, HD), HD)], w_all.at[i, :, HD:2 * HD], w_sem.at[i % ahead]
            ),
        ]
        q = [
            pltpu.make_async_copy(
                wq_any.at[:, pl.ds(pl.multiple_of(c * wide, HD), wide)], w_all.at[i], w_sem.at[i % ahead]
            )
        ]
        return kv, q

    def is_kv(i):
        keys_first = climbs | spread
        return ((i < heads) & keys_first) | ((i >= heads) & jnp.logical_not(keys_first))

    def fetch(i):
        kv, q = weight_copies(i)

        @pl.when(is_kv(i))
        def _():
            for copy in kv:
                copy.start()

        @pl.when(jnp.logical_not(is_kv(i)))
        def _():
            for copy in q:
                copy.start()

    for i in range(ahead):
        fetch(i)

    asked[...] = jnp.zeros_like(asked)
    asked[0, 0] = asks_ref[...]
    biasv[0] = bias_ref[0]

    @pl.when(climbs)
    def _():
        for d in range(1, layers):
            biasv[d] = bias_ref[d]

    barrier = pltpu.get_barrier_semaphore()
    gated = ((top >= 2) | (top == 0)) & (core + jnp.where(climbs, 1, 0) < shares)
    mate = core + 1 - 2 * (core % 2)
    for share in range(1, shares):
        pl.semaphore_signal(barrier, inc=1, **at(me, (core + share) % shares))

    for m in range(1, plane):
        pl.semaphore_signal(barrier, inc=1, **at(peer(m)))

    @pl.when(below)
    def _():
        pl.semaphore_signal(barrier, inc=1, **at(me - plane))

    @pl.when(sinks)
    def _():
        def greet(device, _):
            pl.semaphore_signal(barrier, inc=1, **at(device))
            return 0

        lax.fori_loop((layer + 1) * plane, layers * plane, greet, 0)

    def tell(d, m):
        return pltpu.make_async_remote_copy(
            src_ref=asks_ref, dst_ref=asked.at[d, m], send_sem=tell_send.at[d], recv_sem=tell_recv.at[d],
            **at((layer - d) * plane + (seat ^ m)),
        )

    def tell_bias(d):
        return pltpu.make_async_remote_copy(
            src_ref=bias_ref.at[d], dst_ref=biasv.at[d], send_sem=bias_send.at[d], recv_sem=bias_recv.at[d],
            **at(me - d * plane),
        )

    def tells(d):
        first = 1 if d == 0 else 0
        span = asked.at[d, first:plane]
        return pltpu.make_async_remote_copy(
            src_ref=span, dst_ref=span, send_sem=tell_send.at[d], recv_sem=tell_recv.at[d], **at(me - d * plane)
            if d else at(peer(1)),
        )

    def each_tell(far, act, bias_act):
        act(0)
        for d in range(1, layers):
            @pl.when(sinks & far(d))
            def _():
                act(d)
                bias_act(d)

    def tell_all(d):
        for m in range(1 if d == 0 else 0, plane):
            tell(d, m).start()

    def climb(d, c):
        return pltpu.make_async_remote_copy(
            src_ref=held.at[d, c], dst_ref=held.at[d + 1, c],
            send_sem=flow_send.at[d], recv_sem=flow_recv.at[d, c], **at(me + plane),
        )

    def sink(d, c):
        return pltpu.make_async_remote_copy(
            src_ref=qb.at[d, c], dst_ref=qb.at[d + 1, c],
            send_sem=flow_send.at[d], recv_sem=flow_recv.at[d, c], **at(me - plane),
        )

    def lift(d, c):
        return [
            pltpu.make_async_remote_copy(
                src_ref=up.at[d, c], dst_ref=down.at[d - 1, c],
                send_sem=lift_send.at[d, n], recv_sem=lift_recv.at[d - 1, c, n], **at(me + plane),
            )
            for n, (up, down) in enumerate(((up_o, down_o), (up_s, down_s)))
        ]

    def side(d, c, m):
        return pltpu.make_async_remote_copy(
            src_ref=stage.at[d, c, (m - 1) * CAP:m * CAP], dst_ref=picked.at[d, c, m * CAP:(m + 1) * CAP],
            send_sem=side_send.at[d], recv_sem=side_recv.at[d, c], **at(peer(m)),
        )

    def sides(d, c):
        return pltpu.make_async_remote_copy(
            src_ref=stage.at[d, c], dst_ref=picked.at[d, c, CAP:plane * CAP],
            send_sem=side_send.at[d], recv_sem=side_recv.at[d, c], **at(peer(1)),
        )

    def gather(m, c):
        return pltpu.make_async_remote_copy(
            src_ref=held.at[0, c], dst_ref=held.at[m, c],
            send_sem=side_send.at[m], recv_sem=side_recv.at[m, c], **at(peer(m)),
        )

    def project(i):
        mine = is_kv(i)
        c = i % heads

        pltpu.make_async_copy(w_all.at[i], w_all.at[i], w_sem.at[i % ahead]).wait()

        @pl.when(i + ahead < 2 * heads)
        def _():
            fetch(i + ahead)

        total = None
        for s in range(shares):
            owner = (core + s) % shares
            term = jnp.dot(
                parts[s][...], w_all[i, pl.ds(pl.multiple_of(owner * depth, depth), depth), :],
                preferred_element_type=jnp.float32,
            )
            total = term if total is None else total + term
        total = total.astype(jnp.bfloat16)

        @pl.when(mine)
        def _():
            held[0, c] = total.reshape(own_blocks, BLK, 2 * HD)

        @pl.when(jnp.logical_not(mine))
        def _():
            for g in range(group):
                qb[0, c, g * tok_rows:(g + 1) * tok_rows] = total[:, g * HD:(g + 1) * HD]

    def launch(c):
        @pl.when(climbs & above)
        def _():
            climb(0, c).start()

        if layers >= plane:
            @pl.when(spread)
            def _():
                for m in range(1, plane):
                    gather(m, c).start()

        @pl.when(sinks & below & ((top == 0) | (c < sent)))
        def _():
            sink(0, c).start()

    project(0)

    pl.semaphore_wait(barrier, shares + plane - 2 + above.astype(jnp.int32) + jnp.where(sinks, layer * plane, 0))
    each_tell(lambda d: d <= layer, tell_all, lambda d: tell_bias(d).start())
    launch(0)

    def first_half(i, _):
        project(i)
        launch(i)
        return 0

    lax.fori_loop(1, heads, first_half, 0)

    def second_half(i, _):
        project(i)
        return 0

    lax.fori_loop(heads, 2 * heads, second_half, 0)
    fetch_out = pltpu.make_async_copy(wo_any, wo, wo_sem)
    fetch_out.start()
    acc[...] = jnp.zeros_like(acc)

    def attend(c, where_q, keys, values, mask):
        spans = [slice(g * tok_rows, (g + 1) * tok_rows) for g in range(group)]
        raw = [lax.dot_general(keys, qb[where_q, c, span], NT, preferred_element_type=jnp.float32) for span in spans]
        rounded = []
        for span, s in zip(spans, raw):
            s = mask(s.reshape(-1, BLK, tok_rows))
            peak = jnp.max(jnp.max(s, axis=0), axis=0, keepdims=True)
            p = jnp.exp2((s - peak[None]) * SCALE)
            fr_s[0:1, span] = peak
            fr_s[1:2, span] = jnp.sum(jnp.sum(p, axis=0), axis=0, keepdims=True)
            rounded.append(p.astype(jnp.bfloat16).reshape(-1, tok_rows))
        for span, p in zip(spans, rounded):
            fr_o[:, span] = lax.dot_general(values, p, TN, preferred_element_type=jnp.float32)

    def merge(o_a, s_a, o_b, s_b):
        peak = jnp.maximum(s_a[0:1], s_b[0:1])
        fac_a = jnp.exp2((s_a[0:1] - peak) * SCALE)
        fac_b = jnp.exp2((s_b[0:1] - peak) * SCALE)
        total = s_a[1:2] * fac_a + s_b[1:2] * fac_b
        return o_a.astype(jnp.float32) * fac_a + o_b * fac_b, peak, total

    def put(o_ref, s_ref, value):
        o, peak, total = value
        o_ref[...] = o.astype(o_ref.dtype)
        s_ref[0:1] = peak
        s_ref[1:2] = total

    def local(c):
        key_at = lax.broadcasted_iota(jnp.int32, (own_blocks, BLK, tok_rows), 0) * BLK + lax.broadcasted_iota(
            jnp.int32, (own_blocks, BLK, tok_rows), 1
        )
        query_at = lax.broadcasted_iota(jnp.int32, (own_blocks, BLK, tok_rows), 2)
        own_bias = own_bias_ref[0:own_blocks]

        def mask(s):
            return jnp.where(key_at > query_at, LOW, s + own_bias[:, None, :])

        attend(
            c, 0, held[0, c, :, :, 0:HD].reshape(tok_rows, HD), held[0, c, :, :, HD:2 * HD].reshape(tok_rows, HD), mask
        )
        st_o[c] = fr_o[...]
        st_s[c] = fr_s[...]

    def choose(source, c, block):
        taken = held[source, c, 0]
        for other in range(1, own_blocks):
            taken = jnp.where(block == other, held[source, c, other], taken)
        return taken

    def distribute(d, c):
        source = jnp.where(climbs, d, 0)
        table = jnp.where(climbs, 0, d)
        for m in range(1, plane):
            for place in range(CAP):
                stage[d, c, (m - 1) * CAP + place] = choose(source, c, asked_s[table, m, 0, (d * plane + m) * CAP + place])
            side(d, c, m).start()
        for place in range(CAP):
            picked[d, c, place] = choose(source, c, asked_s[table, 0, 0, d * plane * CAP + place])

    def turn(n):
        i = n // heads
        c = n % heads
        k = n - heads * (top - 1)
        paired = (k >= 0) & below & (top > 1)
        d = top - i
        d = jnp.where(paired, jnp.where(k % 2 == 0, 1, 0), d)
        c = jnp.where(paired, k // 2, c)
        if early > 0:
            m = n - early
            k = m - heads * (top - 2)
            low = jnp.where(k % 2 == 0, 2, 0)
            low = jnp.where((m < 0) | (k >= 2 * heads), 1, jnp.where(k >= 0, low, top - m // heads))
            at_low = jnp.where(k >= 2 * heads, k - 2 * heads + early, jnp.where(k >= 0, k // 2, m % heads))
            d = jnp.where(bottom, low, d)
            c = jnp.where(bottom, jnp.where(m < 0, n, at_low), c)
        return d, c

    busy = sinks & (top > 0)

    def pass_on(d, c):
        sink(d - 1, c).wait_recv()
        sink(d, c).start()

    def ready(c, _):
        @pl.when((busy & (c < jnp.where(top == 1, 1, top + 1) * heads)) | (climbs & (top == 0) & (c < heads)))
        def _():
            d, at_head = turn(c)

            @pl.when(jnp.logical_not(spread))
            def _():
                distribute(jnp.where(climbs, 0, d), jnp.where(climbs, c, at_head))

        return 0

    def to_scalars(first, last):
        move = pltpu.make_async_copy(asked.at[first:last], asked_s.at[first:last], move_sem)
        move.start()
        move.wait()

    tells(0).wait_recv()
    to_scalars(0, 1)

    @pl.when(sinks)
    def _():
        for d in range(1, layers):
            @pl.when(d <= top)
            def _():
                tells(d).wait_recv()
                tell_bias(d).wait_recv()

        if layers > 1:
            to_scalars(1, layers)

    lax.fori_loop(0, layers * heads, ready, 0)

    def forward(i, c):
        @pl.when(climbs & (i >= 1) & (i <= layer))
        def _():
            climb(i - 1, c).wait_recv()

            @pl.when(above)
            def _():
                climb(i, c).start()

        d = top - i

        @pl.when(sinks & below & (d >= 1))
        def _():
            pass_on(d, c)

        @pl.when(sinks & below & (d == 0) & (c == 0) & (top > 0))
        def _():
            def send(n, _):
                sink(0, n).start()
                return 0

            lax.fori_loop(sent, heads, send, 0)

    def finish(c):
        @pl.when(sinks & below)
        def _():
            for copy in lift(1, c):
                copy.wait_recv()
            put(st_o.at[c], st_s.at[c], merge(down_o[0, c], down_s[0, c], st_o[c], st_s[c]))

        for g in range(group):
            span = slice(g * tok_rows, (g + 1) * tok_rows)
            o = st_o[c, :, span] / st_s[c, 1:2, span]
            ho[0, c, :, g * HD:(g + 1) * HD] = o.T.astype(jnp.bfloat16)

        for share in range(1, shares):
            give(share, c).start()

    def give(share, c):
        return pltpu.make_async_remote_copy(
            src_ref=ho.at[0, c], dst_ref=ho.at[share, c],
            send_sem=give_send.at[share], recv_sem=give_recv.at[share, c], **at(me, (core + shares - share) % shares),
        )

    wide = group * HD
    out_cols = out_vmem.shape[1]
    tile = min(256, out_cols)

    def mixed_in(share, c, first):
        owner = (core + share) % shares
        rows_of = pl.multiple_of((owner * heads + c) * wide, wide)
        return jnp.dot(
            ho[share, c], wo[pl.ds(rows_of, wide), first:first + tile], preferred_element_type=jnp.float32
        )

    def add_in(c):
        for first in range(0, out_cols, tile):
            acc[:, first:first + tile] += mixed_in(0, c, first)

    def wait_blocks(d, c, fresh):
        if layers >= plane:
            @pl.when(spread)
            def _():
                @pl.when(fresh)
                def _():
                    for m in range(1, plane):
                        gather(m, c).wait_recv()

                for m in range(plane):
                    for place in range(CAP):
                        picked[d, c, m * CAP + place] = choose(m, c, asked_s[d, 0, 0, (d * plane + m) * CAP + place])

        @pl.when(jnp.logical_not(spread))
        def _():
            sides(d, c).wait_recv()

    def compute(d, c, fresh):
        away = sinks & (d >= 1)

        @pl.when(away & jnp.logical_not(below))
        def _():
            sink(d - 1, c).wait_recv()

        wait_blocks(d, c, fresh)
        group_bias = biasv[d]
        attend(
            c, jnp.where(climbs, 0, d),
            picked[d, c, :, :, 0:HD].reshape(cands * BLK, HD), picked[d, c, :, :, HD:2 * HD].reshape(cands * BLK, HD),
            lambda s: s + group_bias[:, None, :],
        )

        @pl.when(away)
        def _():
            @pl.when(below)
            def _():
                for copy in lift(d + 1, c):
                    copy.wait_recv()
                put(up_o.at[d, c], up_s.at[d, c], merge(down_o[d, c], down_s[d, c], fr_o[...], fr_s[...]))

            @pl.when(jnp.logical_not(below))
            def _():
                up_o[d, c] = fr_o[...].astype(jnp.bfloat16)
                up_s[d, c] = fr_s[...]

            for copy in lift(d, c):
                copy.start()

        @pl.when(jnp.logical_not(away))
        def _():
            put(st_o.at[c], st_s.at[c], merge(st_o[c], st_s[c], fr_o[...], fr_s[...]))

            @pl.when(climbs & (d == layer))
            def _():
                finish(c)
                add_in(c)

    hold = jnp.where(climbs, jnp.where(top >= 2, 2, jnp.where(above, 1, 0)), jnp.where((top == 0) & below, 1, 0))
    lag = jnp.where(bottom, 0, hold + jnp.where(climbs & (top == 1), 2, 1)) * heads
    fetch_out.wait()

    def step(n, _):
        i = n // heads
        c = n % heads

        @pl.when(i < layers)
        def _():
            forward(i, c)

        due = i - hold

        waits = gated & (climbs ^ (top == 0))

        @pl.when(waits & (n == hold * heads))
        def _():
            pl.semaphore_wait(go_sem, 1)

        @pl.when(gated & jnp.logical_not(waits) & (n == jnp.where(climbs, 3 * heads - heads // 2, jnp.where(below, 1, heads + heads // 4))))
        def _():
            pl.semaphore_signal(go_sem, inc=1, **at(me, mate))

        first_due = jnp.where(above, 0, 1)

        @pl.when((climbs & (due >= first_due) & (due <= layer)) | (sinks & (top == 0) & (due == 0)))
        def _():
            distribute(due, c)

        @pl.when(sinks & (top == 1) & (n == heads))
        def _():
            def each(h, _):
                distribute(0, h)
                return 0

            lax.fori_loop(0, heads, each, 0)

        @pl.when((i == 0) & jnp.logical_not(bottom))
        def _():
            local(c)

        @pl.when(bottom & (n == early))
        def _():
            def each(h, _):
                local(h)
                return 0

            lax.fori_loop(0, heads, each, 0)

        late = n - lag

        @pl.when((late >= 0) & (late < jnp.where(climbs, layer + 1, top + 1) * heads))
        def _():
            d, at_head = turn(late)
            fresh = (late < early) | ((late >= 2 * early) & (late < early + heads))
            compute(jnp.where(climbs, late // heads, d), jnp.where(climbs, late % heads, at_head), fresh)

        return 0

    lax.fori_loop(0, (layers + 3) * heads, step, 0)

    @pl.when(sinks)
    def _():
        def last(c, _):
            finish(c)
            add_in(c)
            return 0

        lax.fori_loop(0, heads, last, 0)

    def other(n, _):
        share = 1 + n // heads
        c = n % heads
        give(share, c).wait_recv()
        for first in range(0, out_cols, tile):
            acc[:, first:first + tile] += mixed_in(share, c, first)
        return 0

    total = (shares - 1) * heads
    final = [(1 + n // heads, n % heads) for n in range(max(total - 2, 0), total)]
    lax.fori_loop(0, total - len(final), other, 0)
    for share, c in final:
        give(share, c).wait_recv()
    for first in range(0, out_cols, tile):
        value = acc[:, first:first + tile]
        for share, c in final:
            value = value + mixed_in(share, c, first)
        out_vmem[:, first:first + tile] = value.astype(jnp.bfloat16)

    each_tell(lambda d: d <= layer, lambda d: tells(d).wait_send(), lambda d: tell_bias(d).wait_send())

    def sent_all(ref, sem):
        return pltpu.make_async_remote_copy(src_ref=ref, dst_ref=ref, send_sem=sem, recv_sem=sem, **at(peer(1)))

    def drain(d, _):
        @pl.when((climbs & (d <= layer)) | (sinks & (d <= top)))
        def _():
            @pl.when(jnp.logical_not(spread))
            def _():
                sent_all(stage.at[d], side_send.at[d]).wait_send()

            @pl.when(spread & (d >= 1) & (d < plane))
            def _():
                sent_all(held.at[0], side_send.at[d]).wait_send()

            @pl.when(climbs & above)
            def _():
                sent_all(held.at[d], flow_send.at[d]).wait_send()

            @pl.when(sinks & below)
            def _():
                sent_all(qb.at[d], flow_send.at[d]).wait_send()

            @pl.when(sinks & (d >= 1))
            def _():
                sent_all(up_o.at[d], lift_send.at[d, 0]).wait_send()
                sent_all(up_s.at[d], lift_send.at[d, 1]).wait_send()

        return 0

    lax.fori_loop(0, layers, drain, 0)
    for share in range(1, shares):
        sent_all(ho.at[0], give_send.at[share]).wait_send()


def attention(asks, bias, own_bias, parts, query_weight, key_weight, value_weight, out_weight, plane, layers):
    tok_rows, depth = parts[0].shape
    width, query_cols = query_weight.shape
    cols = key_weight.shape[1]
    heads = cols // HD
    group = query_cols // cols
    rows = group * tok_rows
    own_blocks = tok_rows // BLK
    out_cols = out_weight.shape[1]
    shares = len(parts)
    peers = plane - 1
    lanes = asks.shape[1]
    kind = parts[0].dtype
    dma = pltpu.SemaphoreType.DMA
    return pl.pallas_call(
        functools.partial(attention_kernel, plane, layers, shares),
        out_shape=jax.ShapeDtypeStruct((tok_rows, out_cols), kind),
        in_specs=[pl.BlockSpec(memory_space=VMEM)] * 3 + [pl.BlockSpec(memory_space=pl.ANY)] * 4
        + [pl.BlockSpec(memory_space=VMEM)] * shares,
        out_specs=pl.BlockSpec(memory_space=VMEM),
        scratch_shapes=[
            pltpu.VMEM((layers, heads, own_blocks, BLK, 2 * HD), kind),
            pltpu.VMEM((layers, heads, rows, HD), kind),
            pltpu.VMEM((layers, heads, plane * CAP, BLK, 2 * HD), kind),
            pltpu.VMEM((layers, heads, peers * CAP, BLK, 2 * HD), kind),
            pltpu.VMEM((layers, heads, HD, rows), kind),
            pltpu.VMEM((layers, heads, 2, rows), jnp.float32),
            pltpu.VMEM((layers, heads, HD, rows), kind),
            pltpu.VMEM((layers, heads, 2, rows), jnp.float32),
            pltpu.VMEM((heads, HD, rows), jnp.float32),
            pltpu.VMEM((heads, 2, rows), jnp.float32),
            pltpu.VMEM((HD, rows), jnp.float32),
            pltpu.VMEM((2, rows), jnp.float32),
            pltpu.VMEM((layers, plane, 1, lanes), jnp.int32),
            pltpu.SMEM((layers, plane, 1, lanes), jnp.int32),
            pltpu.VMEM(bias.shape, jnp.float32),
            pltpu.VMEM((2 * heads, width, group * HD), kind),
            pltpu.VMEM(out_weight.shape, kind),
            pltpu.VMEM((shares, heads, tok_rows, group * HD), kind),
            pltpu.VMEM((tok_rows, out_cols), jnp.float32),
            dma((min(3, 2 * heads),)), pltpu.SemaphoreType.REGULAR,
            dma((layers,)), dma((layers,)), dma((layers,)), dma((layers,)), dma(()),
            dma((layers,)), dma((layers, heads)), dma((layers,)), dma((layers, heads)),
            dma((layers, 2)), dma((layers, heads, 2)),
            dma(()), dma((shares,)), dma((shares, heads)),
        ],
        compiler_params=pltpu.CompilerParams(
            collective_id=0, has_side_effects=True, vmem_limit_bytes=51 * 2**20
        ),
    )(asks, bias, own_bias, query_weight, key_weight, value_weight, out_weight, *parts)


def turned(x, shift):
    size = lax.axis_size("tp")
    return lax.ppermute(x, "tp", [((i + shift) % size, i) for i in range(size)])


def shares_of(x):
    size = lax.axis_size("tp")
    me = lax.axis_index("tp")
    return [(x if s == 0 else turned(x, s), (me + s) % size) for s in range(size)]


def tables(chosen, plane, layers):
    own_blocks = chosen.shape[0]
    device = lax.axis_index("kv")
    layer = lax.div(device, jnp.int32(plane))
    seat = device - layer * plane
    holder = lax.div(chosen, jnp.int32(own_blocks))
    within = chosen - holder * own_blocks
    holder_layer = lax.div(holder, jnp.int32(plane))
    owner = (layer - holder_layer) * plane + ((holder - holder_layer * plane) ^ seat)
    count = layers * plane
    ids = jnp.arange(count, dtype=jnp.int32)
    hit = owner.reshape(1, -1) == ids[:, None]
    low = jnp.min(jnp.where(hit, within.reshape(1, -1), own_blocks), axis=1)
    high = jnp.max(jnp.where(hit, within.reshape(1, -1), -1), axis=1)
    asks = jnp.stack([jnp.where(low < own_blocks, low, 0), jnp.maximum(high, 0)], axis=1).reshape(1, -1)
    lanes = -(-asks.shape[1] // 128) * 128
    asks = jnp.pad(asks, ((0, 0), (0, lanes - asks.shape[1])))
    far = ids >= 1
    names = jnp.stack(
        [
            jnp.where(far & (low < own_blocks), ids * own_blocks + low, -1),
            jnp.where(far & (high > low), ids * own_blocks + high, -1),
        ],
        axis=1,
    ).reshape(-1)
    names = jnp.concatenate([names, jnp.arange(8, dtype=jnp.int32)])
    wanted = jnp.repeat(jnp.transpose(owner * own_blocks + within), BLK, axis=1)
    seen = jnp.any(wanted[None] == names[:, None, None], axis=1)
    bias = jnp.where(seen, 0.0, LOW).astype(jnp.float32)
    cut = count * CAP
    return asks, bias[:cut].reshape(layers, plane * CAP, -1), bias[cut:]


def local(tokens, query_weight, key_weight, value_weight, out_weight, chosen):
    key_devices = lax.axis_size("kv")
    plane = math.gcd(key_devices, PLANE)
    layers = key_devices // plane
    asks, bias, own_bias = tables(chosen, plane, layers)
    parts = [block for block, _ in shares_of(tokens)]
    return attention(
        asks, bias, own_bias, parts, query_weight, key_weight, value_weight, out_weight, plane, layers
    )


def solution(mesh):
    return jax.shard_map(
        local,
        mesh=mesh,
        in_specs=(
            P("kv", "tp"),
            P(None, "tp"),
            P(None, "tp"),
            P(None, "tp"),
            P(None, "tp"),
            P("kv", None),
        ),
        out_specs=P("kv", "tp"),
        check_vma=False,
    )
```
